256 devices in a mesh: sp: 32 (over z, x), tp: 8 (over y, core).
Axes of the slice: x: 4, y: 4, z: 8, core: 2. Of those that a mesh axis runs over, the one named last changes fastest.
Arguments:
- tokens: bfloat16 [32768, 2048], P('sp', 'tp'), may hold values from -70 to 70
- w_query: bfloat16 [2048, 1024], P(None, 'tp'), may hold values from -0.125 to 0.125
- w_key: bfloat16 [2048, 1024], P(None, 'tp'), may hold values from -0.125 to 0.125
- w_value: bfloat16 [2048, 1024], P(None, 'tp'), may hold values from -0.125 to 0.125
- w_delta_gate: bfloat16 [2048, 1024], P(None, 'tp'), may hold values from -0.125 to 0.125
- w_glu_value: bfloat16 [2048, 1024], P(None, 'tp'), may hold values from -0.125 to 0.125
- w_glu_gate: bfloat16 [2048, 1024], P(None, 'tp'), may hold values from -0.125 to 0.125
- w_conv_gate: bfloat16 [2048, 1024], P(None, 'tp'), may hold values from -0.125 to 0.125
- w_beta: bfloat16 [2048, 8], replicated, may hold values from -0.125 to 0.125
- w_decay: bfloat16 [2048, 8], replicated, may hold values from -0.125 to 0.125
- decay_log: float32 [8], replicated, may hold values from -12 to -3
- head_gain: float32 [128], replicated, may hold values from 0.1 to 1.9
- conv_taps: bfloat16 [31, 1024], P(None, 'tp'), may hold values from -2.5 to 2.5
- ln_gain: float32 [1024], P('tp'), may hold values from 0.1 to 1.9
- ln_shift: float32 [1024], P('tp'), may hold values from -3 to 3
- out_delta: bfloat16 [1024, 2048], P('tp'), may hold values from -0.125 to 0.125
- out_conv: bfloat16 [1024, 2048], P('tp'), may hold values from -0.125 to 0.125
Outputs:
- mixed_out: bfloat16 [32768, 2048], P(('sp', 'tp'))
The draws below stay inside these ranges and needn't reach their ends.
All inputs are finite; a program needn't handle non-finite values.
Results may differ from the reference program's by a relative error of at most 0.024.
Values may be sent and summed in bfloat16 or wider, within the bound.
A program may use at most 64 MiB of HBM per device.

```python
import jax
import jax.numpy as jnp
from jax import lax

D = 2048
HEADS = 8
DK = 128
CV = 1024
KERNEL = 31
SPAN = 64
TOKENS = 32768
N_TP = 8


def draw_tokens(key, part):
    keys = jax.random.split(key, 3)
    span_rows = 4 * SPAN
    groups = (TOKENS + span_rows - 1) // span_rows
    shifts = jnp.clip(jax.random.normal(keys[1], (groups, D), jnp.float32), -6.0, 6.0) * 1.5
    shifts = jnp.repeat(shifts, span_rows, axis=0)[:TOKENS]
    noise = jnp.clip(jax.random.normal(keys[0], (TOKENS, D), jnp.float32), -6.0, 6.0)
    spread = 0.7
    scales = jnp.exp(jax.random.uniform(keys[2], (TOKENS, 1), jnp.float32, -spread, spread))
    return ((noise + shifts) * scales).astype(jnp.bfloat16)


def draw_decay_log(key, part):
    keys = jax.random.split(key, 3)
    order = jax.random.permutation(keys[0], HEADS)
    fast_heads = HEADS // 2
    slow_rate = jax.random.uniform(keys[1], (HEADS,), jnp.float32, 0.3, 1.0) * 2.3 / TOKENS
    fast_rate = jax.random.uniform(keys[2], (HEADS,), jnp.float32, 0.015, 0.04)
    return jnp.log(jnp.where(order < fast_heads, fast_rate, slow_rate)).astype(jnp.float32)


def draw_conv_taps(key, part):
    keys = jax.random.split(key, 2)
    noise = jnp.clip(jax.random.normal(keys[0], (KERNEL, CV), jnp.float32), -4.0, 4.0)
    spread = 1.2
    levels = jnp.exp(jax.random.uniform(keys[1], (16,), jnp.float32, -spread, spread))
    group_ids = jnp.arange(CV) * 16 // CV
    column_scale = jnp.take(levels, group_ids)
    return (noise * column_scale[None, :] * KERNEL ** (-0.5)).astype(jnp.bfloat16)


def level_of(key, shape, shards, smallest, high):
    def one(axis_at, shards_of):
        heights = jax.random.uniform(jax.random.fold_in(jax.random.fold_in(key, 6), axis_at), (shards_of,), jnp.float32, smallest / len(shards), high / len(shards))
        return jnp.repeat(jnp.exp(heights), shape[axis_at] // shards_of).reshape((-1,) + (1,) * (len(shape) - axis_at - 1))

    loudness = one(*shards[0])
    for cut in shards[1:]:
        loudness = loudness * one(*cut)
    return loudness


def gaussian(own_key, shape, scale, reach, shards=(), kind=jnp.bfloat16):
    entries = scale * jax.random.normal(own_key, shape, jnp.float32)
    if shards:
        entries = entries * level_of(own_key, shape, shards, -0.22, 0.18)
    return jnp.clip(entries, -reach, reach).astype(kind)


def setup_inputs(seed: int = 0) -> dict:
    splits = jax.random.split(jax.random.key(seed), 18)
    tokens = draw_tokens(jax.random.fold_in(splits[17], 71), 0)
    w_query = gaussian(splits[1], (D, HEADS * DK), D ** -0.5, 0.125, ((1, 8),))
    w_key = gaussian(splits[2], (D, HEADS * DK), D ** -0.5, 0.125, ((1, 8),))
    w_value = gaussian(splits[3], (D, HEADS * DK), D ** -0.5, 0.125, ((1, 8),))
    w_delta_gate = gaussian(splits[4], (D, HEADS * DK), D ** -0.5, 0.125, ((1, 8),))
    w_glu_value = gaussian(splits[5], (D, CV), D ** -0.5, 0.125, ((1, 8),))
    w_glu_gate = gaussian(splits[6], (D, CV), D ** -0.5, 0.125, ((1, 8),))
    w_conv_gate = gaussian(splits[7], (D, CV), D ** -0.5, 0.125, ((1, 8),))
    w_beta = gaussian(splits[8], (D, HEADS), D ** -0.5, 0.125)
    w_decay = gaussian(splits[9], (D, HEADS), D ** -0.5, 0.125)
    decay_log = draw_decay_log(jax.random.fold_in(splits[17], 71), 0)
    head_gain = jnp.clip(1.0 + 0.18 * jax.random.normal(splits[11], (DK,), jnp.float32), 0.1, 1.9)
    conv_taps = draw_conv_taps(jax.random.fold_in(splits[17], 71), 0)
    ln_gain = jnp.clip(1.0 + 0.18 * jax.random.normal(splits[13], (CV,), jnp.float32), 0.1, 1.9)
    ln_shift = gaussian(splits[14], (CV,), 0.5, 3.0, ((0, 8),), jnp.float32)
    out_delta = gaussian(splits[15], (HEADS * DK, D), (HEADS * DK + CV) ** -0.5, 0.125, ((0, 8),))
    out_conv = gaussian(splits[16], (CV, D), (HEADS * DK + CV) ** -0.5, 0.125, ((0, 8),))
    return {"tokens": tokens, "w_query": w_query, "w_key": w_key, "w_value": w_value, "w_delta_gate": w_delta_gate, "w_glu_value": w_glu_value, "w_glu_gate": w_glu_gate, "w_conv_gate": w_conv_gate, "w_beta": w_beta, "w_decay": w_decay, "decay_log": decay_log, "head_gain": head_gain, "conv_taps": conv_taps, "ln_gain": ln_gain, "ln_shift": ln_shift, "out_delta": out_delta, "out_conv": out_conv}


TINY_NORM = 1e-06
TINY_VAR = 1e-05
HIGHEST = lax.Precision.HIGHEST

def head_rule(query, keys, values, strength, log_decay):
    blocks = query.shape[0] // SPAN

    def split_blocks(array):
        return array.reshape((blocks, SPAN) + array.shape[1:])
    query, keys, values = (split_blocks(query), split_blocks(keys), split_blocks(values))
    strength, log_decay = (split_blocks(strength), split_blocks(log_decay))
    log_sum = jnp.cumsum(log_decay, axis=-1)
    offsets = jnp.arange(SPAN)
    causal = offsets[:, None] >= offsets[None, :]
    strict = offsets[:, None] > offsets[None, :]
    spread = log_sum[:, :, None] - log_sum[:, None, :]
    damping = jnp.where(causal, jnp.exp(jnp.where(causal, spread, 0.0)), 0.0)
    scaled_keys = keys * strength[..., None]
    lower = jnp.where(strict, jnp.einsum('nid,njd->nij', scaled_keys, keys, precision=HIGHEST) * damping, 0.0)
    identity = jnp.eye(SPAN, dtype=jnp.float32)
    right = jnp.concatenate([values * strength[..., None], scaled_keys * jnp.exp(log_sum)[..., None]], axis=-1)
    solved = jax.scipy.linalg.solve_triangular(identity + lower, right, lower=True, unit_diagonal=True)
    width = values.shape[-1]
    corrected = solved[..., :width]
    key_terms = solved[..., width:]
    scores = jnp.einsum('nid,njd->nij', query, keys, precision=HIGHEST) * damping

    def advance(memory, inputs):
        query_block, keys_block, corrected_block, terms_block, scores_block, log_block = inputs
        fresh = corrected_block - jnp.dot(terms_block, memory, precision=HIGHEST)
        output = jnp.dot(query_block * jnp.exp(log_block)[:, None], memory, precision=HIGHEST)
        output = output + jnp.dot(scores_block, fresh, precision=HIGHEST)
        tail_log = log_block[-1]
        weighted = keys_block * jnp.exp(tail_log - log_block)[:, None]
        memory = memory * jnp.exp(tail_log) + jnp.dot(weighted.T, fresh, precision=HIGHEST)
        return (memory, output)
    start = jnp.zeros((keys.shape[-1], width), jnp.float32)
    ignored, outputs = lax.scan(advance, start, (query, keys, corrected, key_terms, scores, log_sum))
    return outputs.reshape(blocks * SPAN, width)

def reference(tokens, w_query, w_key, w_value, w_delta_gate, w_glu_value, w_glu_gate, w_conv_gate, w_beta, w_decay, decay_log, head_gain, conv_taps, ln_gain, ln_shift, out_delta, out_conv):
    length = tokens.shape[0]
    floats = tokens.astype(jnp.float32)
    inv_rms = lax.rsqrt(lax.optimization_barrier(jnp.mean(floats * floats, axis=1, keepdims=True)) + TINY_NORM)

    def project(weight):
        return jnp.dot(tokens.astype(jnp.float32), weight.astype(jnp.float32), preferred_element_type=jnp.float32) * inv_rms
    query_raw = project(w_query).astype(jnp.bfloat16)
    key_raw = project(w_key).astype(jnp.bfloat16)
    value_raw = project(w_value).astype(jnp.bfloat16)
    delta_gate_raw = project(w_delta_gate).astype(jnp.bfloat16)
    glu_value_raw = project(w_glu_value).astype(jnp.bfloat16)
    glu_gate_raw = project(w_glu_gate).astype(jnp.bfloat16)
    conv_gate_raw = project(w_conv_gate).astype(jnp.bfloat16)
    strength = jax.nn.sigmoid(project(w_beta))
    log_decay = -jnp.exp(decay_log)[None, :] * jax.nn.softplus(project(w_decay))

    def to_heads(raw):
        return raw.astype(jnp.float32).reshape(length, HEADS, DK)

    def unit_rows(array):
        return array * lax.rsqrt(lax.optimization_barrier(jnp.sum(array * array, axis=-1, keepdims=True)) + TINY_NORM)
    query = unit_rows(to_heads(query_raw)) * DK ** (-0.5)
    keys = unit_rows(to_heads(key_raw))
    values = to_heads(value_raw)
    heads_out = lax.map(lambda inputs: head_rule(*inputs), (jnp.moveaxis(query, 1, 0), jnp.moveaxis(keys, 1, 0), jnp.moveaxis(values, 1, 0), strength.T, log_decay.T))
    output = jnp.moveaxis(heads_out, 0, 1)
    output = output * lax.rsqrt(lax.optimization_barrier(jnp.mean(output * output, axis=-1, keepdims=True)) + TINY_NORM) * head_gain
    delta_mixed = (output.reshape(length, HEADS * DK) * jax.nn.silu(delta_gate_raw.astype(jnp.float32))).astype(jnp.bfloat16)
    gated_units = (glu_value_raw.astype(jnp.float32) * jax.nn.sigmoid(glu_gate_raw.astype(jnp.float32))).astype(jnp.bfloat16)
    padded = jnp.concatenate([jnp.zeros((KERNEL - 1, CV), jnp.bfloat16), gated_units], axis=0)
    filtered = jnp.zeros((length, CV), jnp.float32)
    for offset in range(KERNEL):
        filtered = filtered + padded[offset:offset + length].astype(jnp.float32) * conv_taps[offset].astype(jnp.float32)
    center = lax.optimization_barrier(jnp.sum(filtered, axis=1)) / CV
    variance = jnp.maximum(lax.optimization_barrier(jnp.sum(filtered * filtered, axis=1)) / CV - center * center, 0.0)
    normed = (filtered - center[:, None]) * lax.rsqrt(variance + TINY_VAR)[:, None] * ln_gain + ln_shift
    conv_mixed = (jax.nn.silu(normed) * jax.nn.silu(conv_gate_raw.astype(jnp.float32))).astype(jnp.bfloat16)
    head_block = HEADS * DK // N_TP
    chan_block = CV // N_TP
    summed = jnp.zeros((length, D), jnp.float32)
    for group in range(N_TP):
        partial_value = jnp.dot(delta_mixed[:, group * head_block:(group + 1) * head_block].astype(jnp.float32), out_delta[group * head_block:(group + 1) * head_block].astype(jnp.float32), preferred_element_type=jnp.float32)
        partial_value = partial_value + jnp.dot(conv_mixed[:, group * chan_block:(group + 1) * chan_block].astype(jnp.float32), out_conv[group * chan_block:(group + 1) * chan_block].astype(jnp.float32), preferred_element_type=jnp.float32)
        partial_value = lax.optimization_barrier(partial_value.astype(jnp.bfloat16))
        summed = summed + partial_value.astype(jnp.float32)
    return summed.astype(jnp.bfloat16)
```

```python
import jax
import jax.numpy as jnp
from jax import lax
from jax.experimental import pallas as pl
from jax.experimental.pallas import tpu as pltpu
from jax.sharding import PartitionSpec as P

BF = jnp.bfloat16
F32 = jnp.float32
ROWS = 1024
SHARD = 256
BLK = 128
CHUNK = 512
CHUNKS = ROWS // CHUNK
HALF = CHUNK // 2
PER = CHUNK // BLK
COLS = 9 * 128
TAPS = 31
NORM = 1e-06
VAR = 1e-05
NN = ((1,), (0,))
NT = ((1,), (1,))
TN = ((0,), (0,))


def mm(a, b, dims=NN):
    return lax.dot_general(
        a.astype(BF), b.astype(BF), (dims, ((), ())), preferred_element_type=F32
    )


def iotas(shape):
    return lax.broadcasted_iota(jnp.int32, shape, 0), lax.broadcasted_iota(jnp.int32, shape, 1)


def softplus(v):
    return jnp.maximum(v, 0.0) + jnp.log1p(jnp.exp(-jnp.abs(v)))


def sigmoid(v):
    return jax.nn.sigmoid(v)


def unit_rows(v):
    return v * lax.rsqrt(jnp.sum(v * v, axis=-1, keepdims=True) + NORM)


def block_inverse(lows):
    row, col = iotas((BLK, BLK))
    eye = (row == col).astype(F32)
    parts = [eye - jnp.where((row // 2 == col // 2), low, 0.0) for low in lows]
    m = 2
    while m < BLK:
        pick = (row // (2 * m) == col // (2 * m)) & (row // m != col // m)
        packed = [p.astype(BF) for p in parts]
        inner = [mm(jnp.where(pick, low, 0.0), p) for low, p in zip(lows, packed)]
        parts = [t - mm(p, i) for t, p, i in zip(parts, packed, inner)]
        m *= 2
    return parts


def kernel(
    x, wq, wk, wv, wdg, wgv, wgg, wcg, wb, wd, dlog, hgain, taps, lng, lns, od, oc,
    out,
    xg, w, wo, qs, ks, vs, dgs, cgs, bes, lds, pad, filt, qcs, ocs, mn, mnx, mnz, s4s, s4r,
    halo_s, halo_r, sts, str_, dms, cms, dmr, cmr,
    wsem, gs, gr, os_, or_, xs, xr, zs, zr, fs, fr, hs, hr, ss, sr, ds_, dr, cs, cr,
):
    sp = lax.axis_index("sp")
    t = lax.axis_index("tp")
    y, c = t // 2, t % 2
    z, xx = sp // 4, sp % 4
    zq, zi = z // 4, z % 4
    right = ((y + 1) % 4) * 2 + c
    left = ((y + 3) % 4) * 2 + c
    opp = ((y + 2) % 4) * 2 + c
    mate = y * 2 + (1 - c)

    def at_tp(k):
        return {"sp": sp, "tp": k}

    def at_sp(k):
        return {"sp": k, "tp": t}

    wrefs = (wq, wk, wv, wdg, wgv, wgg, wcg)
    wcopies = [
        pltpu.make_async_copy(ref, w.at[:, k * 128 : (k + 1) * 128], wsem.at[k])
        for k, ref in enumerate(wrefs)
    ]
    own_rows = pl.ds(pl.multiple_of(t * 128, 128), 128)
    wcopies.append(pltpu.make_async_copy(od, wo.at[0, own_rows, :], wsem.at[7]))
    wcopies.append(pltpu.make_async_copy(oc, wo.at[1, own_rows, :], wsem.at[8]))

    def cols_of(k):
        return pl.ds(pl.multiple_of(k * SHARD, SHARD), SHARD)

    xcopy = pltpu.make_async_copy(x, xg.at[:, cols_of(t)], wsem.at[9])
    xcopy.start()
    for cp in wcopies:
        cp.start()

    bar = pltpu.get_barrier_semaphore()
    peers = [at_tp((t + d) % 8) for d in range(1, 8)]
    peers += [at_sp(z * 4 + (xx + d) % 4) for d in range(1, 4)]
    peers += [at_sp((zq * 4 + (zi + d) % 4) * 4 + xx) for d in range(1, 4)]
    peers += [at_sp(((z + 4) % 8) * 4 + xx), at_sp((sp + 1) % 32), at_sp((sp + 31) % 32)]
    for peer in peers:
        pl.semaphore_signal(bar, inc=1, device_id=peer, device_id_type=pl.DeviceIdType.MESH)
    pl.semaphore_wait(bar, len(peers))

    def send(src, dst, ssem, rsem, to):
        return pltpu.make_async_remote_copy(
            src_ref=src, dst_ref=dst, send_sem=ssem, recv_sem=rsem,
            device_id=to, device_id_type=pl.DeviceIdType.MESH,
        )

    def gat(kind, r):
        base = r * CHUNK
        whole = pl.ds(pl.multiple_of(base, CHUNK), CHUNK)
        first = pl.ds(pl.multiple_of(base, HALF), HALF)
        second = pl.ds(pl.multiple_of(base + HALF, HALF), HALF)
        rows = (whole, whole, whole, first, second, whole, whole, first, second)[kind]
        shard = (t, t, t, left, right, left, right, opp, opp)[kind]
        to = (right, left, mate, right, left, mate, mate, mate, mate)[kind]
        dst = xg.at[rows, cols_of(shard)]
        src = x.at[rows, :] if kind < 3 else dst
        return send(src, dst, gs.at[kind, r], gr.at[kind, r], at_tp(to))

    def own(r):
        for kind in (0, 1, 2):
            gat(kind, r).start()

    def relay1(r):
        gat(0, r).wait_recv()
        gat(3, r).start()
        gat(5, r).start()
        gat(1, r).wait_recv()
        gat(4, r).start()
        gat(6, r).start()

    def relay2(r):
        gat(3, r).wait_recv()
        gat(7, r).start()
        gat(4, r).wait_recv()
        gat(8, r).start()

    def owg(kind):
        shard = (t, t, t, left, right, left, right, opp, opp)[kind]
        to = (right, left, mate, right, left, mate, mate, mate, mate)[kind]
        rows = pl.ds(pl.multiple_of(shard * 128, 128), 128)
        if kind in (3, 7):
            ref = wo.at[1, rows, :]
        elif kind in (4, 8):
            ref = wo.at[0, rows, :]
        else:
            ref = wo.at[:, rows, :]
        return send(ref, ref, os_.at[kind], or_.at[kind], at_tp(to))

    own(0)
    own(1)

    pick = (lax.broadcasted_iota(jnp.int32, (8, 128), 0) == t).astype(BF)
    w[:, 896:1024] = mm(wb[...], pick).astype(BF)
    w[:, 1024:1152] = mm(wd[...], pick).astype(BF)
    rate = jnp.exp(jnp.full((1, 128), dlog[t], F32))
    row, col = iotas((BLK, BLK))
    causal = row >= col
    strict = row > col
    tri = causal.astype(F32)
    mn[:, :128] = (row == col).astype(F32)
    mn[:, 128:] = jnp.zeros((BLK, BLK), F32)

    for cp in wcopies[:7]:
        cp.wait()
    xcopy.wait()

    def project(r):
        for sub in range(CHUNK // 256):
            rows = pl.ds(pl.multiple_of(r * CHUNK + sub * 256, 256), 256)
            xr_ = xg[rows, :]
            xf = xr_.astype(F32)
            inv = lax.rsqrt(jnp.sum(xf * xf, axis=1, keepdims=True) / 2048.0 + NORM)
            raw = []
            for n in range(0, COLS, 256):
                width = min(256, COLS - n)
                d = jnp.dot(xr_, w[:, n : n + width], preferred_element_type=F32) * inv
                for k in range(width // 128):
                    raw.append(d[:, k * 128 : (k + 1) * 128])
            q, k, v, dg, gv, gg, cg = [a.astype(BF).astype(F32) for a in raw[:7]]
            qs[rows, :] = unit_rows(q) * (128.0 ** -0.5)
            ks[rows, :] = unit_rows(k)
            vs[rows, :] = v
            dgs[rows, :] = dg * sigmoid(dg)
            cgs[rows, :] = cg * sigmoid(cg)
            bes[rows, :] = sigmoid(raw[7])
            lds[rows, :] = -rate * softplus(raw[8])
            below = pl.ds(pl.multiple_of(r * CHUNK + sub * 256 + 32, 32), 256)
            pad[below, :] = (gv * sigmoid(gg)).astype(BF).astype(F32)

    def delta(r):
        spans = [pl.ds(pl.multiple_of(r * CHUNK + b * BLK, BLK), BLK) for b in range(PER)]
        sums, lows, scores = [], [], []
        for rows in spans:
            total = lax.dot_general(
                tri, lds[rows, :], (NN, ((), ())),
                precision=lax.Precision.HIGHEST, preferred_element_type=F32,
            )
            spread = total - total.T
            damp = jnp.where(causal, jnp.exp(jnp.where(causal, spread, 0.0)), 0.0)
            kb = ks[rows, :].astype(BF)
            both = mm(jnp.concatenate([kb, qs[rows, :].astype(BF)], axis=0), kb, NT)
            lows.append(jnp.where(strict, both[:BLK] * bes[rows, :] * damp, 0.0))
            scores.append(both[BLK:] * damp)
            sums.append(total)
        inverses = block_inverse(lows)
        later = []
        for rows, total, score, inv in zip(spans, sums, scores, inverses):
            grow = jnp.exp(total)
            kv, be = ks[rows, :], bes[rows, :]
            rhs = jnp.concatenate([vs[rows, :] * be, kv * be * grow], axis=1)
            solved = mm(inv, rhs).astype(BF)
            mixed = mm(score, solved)
            tail = total[BLK - 1 : BLK, :]
            fresh = mm(kv * jnp.exp(tail - total), solved, TN)
            later.append(
                (
                    jnp.concatenate([qs[rows, :] * grow - mixed[:, 128:], fresh[:, 128:]], axis=0),
                    mixed[:, :128], fresh[:, :128], jnp.exp(tail),
                )
            )
        state = mn[...]
        for rows, (lhs, o_here, n_here, fade) in zip(spans, later):
            moved = mm(lhs, state)
            qcs[rows, :] = moved[:BLK, :128]
            ocs[rows, :] = moved[:BLK, 128:] + o_here
            m_next = state[:, :128] * fade - moved[BLK:, :128]
            n_next = state[:, 128:] * fade - moved[BLK:, 128:] + n_here
            state = jnp.concatenate([m_next, n_next], axis=1)
        mn[...] = state

    def compute(r):
        for kind in (2, 5, 6, 7, 8):
            gat(kind, r).wait_recv()
        project(r)
        delta(r)

    relay1(0)
    relay1(1)
    relay2(0)
    for kk in (7, 8):
        wcopies[kk].wait()

    @pl.loop(0, CHUNKS)
    def _(r):
        compute(r)

        @pl.when(r == 0)
        def _():
            relay2(1)

    own_x = mn[...].astype(BF)
    mnx[xx] = own_x

    def xsend(d):
        return send(mnx.at[xx], mnx.at[xx], xs.at[d - 1], xr.at[d - 1],
                    at_sp(z * 4 + (xx + d) % 4))

    for d in (1, 2, 3):
        xsend(d).start()
    halo_s[...] = pad[ROWS : ROWS + 32, :].astype(BF)
    hcopy = send(halo_s, halo_r, hs, hr, at_sp((sp + 1) % 32))
    hcopy.start()
    for kind in (0, 1, 2):
        owg(kind).start()

    tapf = taps[...].astype(F32)

    def conv_rows(i):
        acc = jnp.zeros((64, 128), F32)
        for j in range(TAPS):
            acc = acc + pad[pl.ds(i * 64 + 2 + j, 64), :] * tapf[j : j + 1, :]
        filt[pl.ds(pl.multiple_of(i * 64, 64), 64), :] = acc

    @pl.loop(1, ROWS // 64)
    def _(i):
        conv_rows(i)

    hcopy.wait_recv()
    keep = (sp > 0).astype(F32)
    pad[0:32, :] = halo_r[...].astype(F32) * keep
    conv_rows(0)
    for b in range(ROWS // BLK):
        lanes = slice(b * BLK, (b + 1) * BLK)
        ft = filt[lanes, :].T
        sts[0:1, lanes] = jnp.sum(ft, axis=0, keepdims=True)
        sts[1:2, lanes] = jnp.sum(ft * ft, axis=0, keepdims=True)

    def ssend(d):
        return send(sts, str_.at[t], ss.at[d - 1], sr.at[d - 1], at_tp((t + d) % 8))

    for d in range(1, 8):
        ssend(d).start()
    str_[t] = sts[...]

    def chain(slots, mine):
        total = slots[0].astype(F32)
        m_in = jnp.where(mine > 0, total[:, :128], (row == col).astype(F32))
        n_in = jnp.where(mine > 0, total[:, 128:], 0.0)
        for k in (1, 2, 3):
            piece = slots[k]
            moved = mm(piece[:, :128], total)
            total = jnp.concatenate(
                [moved[:, :128], moved[:, 128:] + piece[:, 128:].astype(F32)], axis=1
            )
            if k < 3:
                m_in = jnp.where(mine > k, total[:, :128], m_in)
                n_in = jnp.where(mine > k, total[:, 128:], n_in)
        return m_in, n_in, total

    for d in (1, 2, 3):
        xsend(d).wait_recv()
    mxp, nxp, xtotal = chain(mnx, xx)
    mnz[zi] = xtotal.astype(BF)

    def zsend(d):
        return send(mnz.at[zi], mnz.at[zi], zs.at[d - 1], zr.at[d - 1],
                    at_sp((zq * 4 + (zi + d) % 4) * 4 + xx))

    for d in (1, 2, 3):
        zsend(d).start()

    owg(0).wait_recv()
    owg(3).start()
    owg(5).start()
    owg(1).wait_recv()
    owg(4).start()
    owg(6).start()

    for d in range(1, 8):
        ssend(d).wait_recv()
    both = str_[0]
    for k in range(1, 8):
        both = both + str_[k]
    center = both[0:1, :] / 1024.0
    variance = jnp.maximum(both[1:2, :] / 1024.0 - center * center, 0.0)
    scale = lax.rsqrt(variance + VAR)
    for b in range(ROWS // BLK):
        lanes = slice(b * BLK, (b + 1) * BLK)
        cen = jnp.broadcast_to(center[:, lanes], (BLK, BLK)).T
        sca = jnp.broadcast_to(scale[:, lanes], (BLK, BLK)).T
        normed = (filt[lanes, :] - cen) * sca * lng[...] + lns[...]
        cms[lanes, :] = (normed * sigmoid(normed) * cgs[lanes, :]).astype(BF)

    def a2a(src, dst, s_sem, r_sem, d):
        to = (t + d) % 8
        rows = pl.ds(pl.multiple_of(to * BLK, BLK), BLK)
        return send(src.at[rows, :], dst.at[t], s_sem.at[d - 1], r_sem.at[d - 1], at_tp(to))

    for d in range(1, 8):
        a2a(cms, cmr, cs, cr, d).start()
    cmr[t] = cms[own_rows, :]

    for d in (1, 2, 3):
        zsend(d).wait_recv()
    mzp, nzp, ztotal = chain(mnz, zi)
    s4s[...] = ztotal[:, 128:].astype(BF)
    fcopy = send(s4s, s4r, fs, fr, at_sp(((z + 4) % 8) * 4 + xx))
    fcopy.start()
    moved = mm(mxp, jnp.concatenate([mzp, nzp], axis=1))
    mpre, npre = moved[:, :128], moved[:, 128:] + nxp
    fcopy.wait_recv()
    begin = s4r[...].astype(F32) * (zq > 0).astype(F32)
    carried = mm(mpre, begin) + npre

    for b in range(ROWS // BLK):
        lanes = slice(b * BLK, (b + 1) * BLK)
        o = ocs[lanes, :] + mm(qcs[lanes, :], carried)
        o = o * lax.rsqrt(jnp.mean(o * o, axis=-1, keepdims=True) + NORM) * hgain[...]
        dms[lanes, :] = (o * dgs[lanes, :]).astype(BF)
    for d in range(1, 8):
        a2a(dms, dmr, ds_, dr, d).start()
    dmr[t] = dms[own_rows, :]

    owg(3).wait_recv()
    owg(7).start()
    owg(4).wait_recv()
    owg(8).start()
    for d in range(1, 8):
        a2a(cms, cmr, cs, cr, d).wait_recv()
    for kind in (2, 5, 6, 7, 8):
        owg(kind).wait_recv()
    for d in range(1, 8):
        a2a(dms, dmr, ds_, dr, d).wait_recv()

    lhs_d = jnp.concatenate([dmr[k] for k in range(8)], axis=1)
    lhs_c = jnp.concatenate([cmr[k] for k in range(8)], axis=1)

    @pl.loop(0, 8)
    def _(n):
        lanes = pl.ds(pl.multiple_of(n * 256, 256), 256)
        acc = jnp.dot(lhs_d, wo[0, :, lanes], preferred_element_type=F32)
        acc = acc + jnp.dot(lhs_c, wo[1, :, lanes], preferred_element_type=F32)
        out[:, lanes] = acc.astype(BF)

    for r in range(CHUNKS):
        for kind in range(9):
            gat(kind, r).wait_send()
    for kind in range(9):
        owg(kind).wait_send()
    for d in (1, 2, 3):
        xsend(d).wait_send()
        zsend(d).wait_send()
    hcopy.wait_send()
    fcopy.wait_send()
    for d in range(1, 8):
        ssend(d).wait_send()
        a2a(cms, cmr, cs, cr, d).wait_send()
        a2a(dms, dmr, ds_, dr, d).wait_send()


def local(*args):
    (tokens, w_query, w_key, w_value, w_delta_gate, w_glu_value, w_glu_gate, w_conv_gate,
     w_beta, w_decay, decay_log, head_gain, conv_taps, ln_gain, ln_shift, out_delta,
     out_conv) = args
    vm = pl.BlockSpec(memory_space=pltpu.VMEM)
    hb = pl.BlockSpec(memory_space=pl.ANY)
    sm = pl.BlockSpec(memory_space=pltpu.SMEM)
    big = lambda kind: pltpu.VMEM((ROWS, 128), kind)
    dma = pltpu.SemaphoreType.DMA
    return pl.pallas_call(
        kernel,
        out_shape=jax.ShapeDtypeStruct((BLK, 2048), BF),
        in_specs=[vm] + [hb] * 7 + [vm, vm, sm] + [vm] * 4 + [hb, hb],
        out_specs=vm,
        scratch_shapes=[
            pltpu.VMEM((ROWS, 2048), BF),
            pltpu.VMEM((2048, COLS), BF),
            pltpu.VMEM((2, 1024, 2048), BF),
            big(F32), big(F32), big(F32), big(F32), big(F32), big(F32), big(F32),
            pltpu.VMEM((ROWS + 32, 128), F32),
            big(F32), big(F32), big(F32),
            pltpu.VMEM((BLK, 256), F32),
            pltpu.VMEM((4, BLK, 256), BF),
            pltpu.VMEM((4, BLK, 256), BF),
            pltpu.VMEM((BLK, BLK), BF),
            pltpu.VMEM((BLK, BLK), BF),
            pltpu.VMEM((32, 128), BF),
            pltpu.VMEM((32, 128), BF),
            pltpu.VMEM((2, ROWS), F32),
            pltpu.VMEM((8, 2, ROWS), F32),
            big(BF), big(BF),
            pltpu.VMEM((8, BLK, BLK), BF),
            pltpu.VMEM((8, BLK, BLK), BF),
            dma((10,)),
            dma((9, CHUNKS)), dma((9, CHUNKS)),
            dma((9,)), dma((9,)),
            dma((3,)), dma((3,)), dma((3,)), dma((3,)),
            dma, dma, dma, dma,
            dma((7,)), dma((7,)), dma((7,)), dma((7,)), dma((7,)), dma((7,)),
        ],
        compiler_params=pltpu.CompilerParams(
            collective_id=0, has_side_effects=True, vmem_limit_bytes=60 * 1024 * 1024
        ),
        name="layer",
    )(
        tokens, w_query, w_key, w_value, w_delta_gate, w_glu_value, w_glu_gate, w_conv_gate,
        w_beta, w_decay, decay_log, head_gain.reshape(1, 128), conv_taps,
        ln_gain.reshape(1, 128), ln_shift.reshape(1, 128), out_delta, out_conv,
    )


def solution(mesh):
    cut = P(None, "tp")
    placed = (P("sp", "tp"),) + (cut,) * 7 + (P(),) * 4 + (
        cut, P("tp"), P("tp"), P("tp", None), P("tp", None),
    )
    return jax.shard_map(
        local, mesh=mesh, in_specs=placed, out_specs=P(("sp", "tp"), None), check_vma=False
    )
```

```python
import jax
import jax.numpy as jnp
from jax import lax
from jax.experimental import pallas as pl
from jax.experimental.pallas import tpu as pltpu
from jax.sharding import PartitionSpec as P

BF = jnp.bfloat16
F32 = jnp.float32
ROWS = 1024
SHARD = 256
BLK = 128
CHUNK = 256
CHUNKS = ROWS // CHUNK
HALF = CHUNK // 2
GROUP = 512
PER = GROUP // BLK
COLS = 8 * 128
MOVES = 31
TAPS = 31
NORM = 1e-06
VAR = 1e-05
NN = ((1,), (0,))
NT = ((1,), (1,))
TN = ((0,), (0,))


def mm(a, b, dims=NN):
    return lax.dot_general(
        a.astype(BF), b.astype(BF), (dims, ((), ())), preferred_element_type=F32
    )


def iotas(shape):
    return lax.broadcasted_iota(jnp.int32, shape, 0), lax.broadcasted_iota(jnp.int32, shape, 1)


def softplus(v):
    return jnp.maximum(v, 0.0) + jnp.log1p(jnp.exp(-jnp.abs(v)))


def sigmoid(v):
    return jax.nn.sigmoid(v)


def unit_rows(v):
    return v * lax.rsqrt(jnp.sum(v * v, axis=-1, keepdims=True) + NORM)


def block_inverse(lows):
    row, col = iotas((BLK, BLK))
    eye = (row == col).astype(F32)
    parts = [eye - jnp.where((row // 2 == col // 2), low, 0.0) for low in lows]
    m = 2
    while m < BLK:
        pick = (row // (2 * m) == col // (2 * m)) & (row // m != col // m)
        packed = [p.astype(BF) for p in parts]
        inner = [mm(jnp.where(pick, low, 0.0), p) for low, p in zip(lows, packed)]
        parts = [t - mm(p, i) for t, p, i in zip(parts, packed, inner)]
        m *= 2
    return parts


def kernel(
    x, wq, wk, wv, wdg, wgv, wgg, wcg, wb, wd, dlog, hgain, taps, lng, lns, od, oc,
    out,
    xg, w, wo, qs, ks, vs, dgs, cgs, bes, lds, pad, filt, qcs, ocs, mn, mnx, mnz, s4s, s4r,
    halo_s, halo_r, sts, str_, dms, cms, dmr, cmr, stage,
    wsem, gs, gr, os_, or_, xs, xr, zs, zr, fs, fr, hs, hr, ss, sr, ds_, dr, cs, cr, osem,
):
    sp = lax.axis_index("sp")
    t = lax.axis_index("tp")
    y, c = t // 2, t % 2
    z, xx = sp // 4, sp % 4
    zq, zi = z // 4, z % 4
    right = ((y + 1) % 4) * 2 + c
    left = ((y + 3) % 4) * 2 + c
    opp = ((y + 2) % 4) * 2 + c
    mate = y * 2 + (1 - c)

    def at_tp(k):
        return {"sp": sp, "tp": k}

    def at_sp(k):
        return {"sp": k, "tp": t}

    wrefs = (wq, wk, wv, wdg, wgv, wgg, wcg)
    wcopies = [
        pltpu.make_async_copy(ref, w.at[:, k * 128 : (k + 1) * 128], wsem.at[k])
        for k, ref in enumerate(wrefs)
    ]
    own_rows = pl.ds(pl.multiple_of(t * 128, 128), 128)
    wcopies.append(pltpu.make_async_copy(od, wo.at[0, own_rows, :], wsem.at[7]))
    wcopies.append(pltpu.make_async_copy(oc, wo.at[1, own_rows, :], wsem.at[8]))

    def cols_of(k):
        return pl.ds(pl.multiple_of(k * SHARD, SHARD), SHARD)

    xcopy = pltpu.make_async_copy(x, xg.at[:, cols_of(t)], wsem.at[9])
    xcopy.start()
    for cp in wcopies:
        cp.start()

    bar = pltpu.get_barrier_semaphore()
    peers = [at_tp((t + d) % 8) for d in range(1, 8)]
    peers += [at_sp(z * 4 + (xx + d) % 4) for d in range(1, 4)]
    peers += [at_sp((zq * 4 + (zi + d) % 4) * 4 + xx) for d in range(1, 4)]
    peers += [at_sp(((z + 4) % 8) * 4 + xx), at_sp((sp + 1) % 32), at_sp((sp + 31) % 32)]
    for peer in peers:
        pl.semaphore_signal(bar, inc=1, device_id=peer, device_id_type=pl.DeviceIdType.MESH)
    pl.semaphore_wait(bar, len(peers))

    def send(src, dst, ssem, rsem, to):
        return pltpu.make_async_remote_copy(
            src_ref=src, dst_ref=dst, send_sem=ssem, recv_sem=rsem,
            device_id=to, device_id_type=pl.DeviceIdType.MESH,
        )

    def gat(kind, r):
        base = r * CHUNK
        whole = pl.ds(pl.multiple_of(base, CHUNK), CHUNK)
        first = pl.ds(pl.multiple_of(base, HALF), HALF)
        second = pl.ds(pl.multiple_of(base + HALF, HALF), HALF)
        rows = (whole, whole, whole, first, second, whole, whole, first, second)[kind]
        shard = (t, t, t, left, right, left, right, opp, opp)[kind]
        to = (right, left, mate, right, left, mate, mate, mate, mate)[kind]
        dst = xg.at[rows, cols_of(shard)]
        return send(dst, dst, gs.at[kind, r], gr.at[kind, r], at_tp(to))

    def own(r):
        for kind in (0, 1, 2):
            gat(kind, r).start()

    def relay1(r):
        gat(0, r).wait_recv()
        gat(3, r).start()
        gat(5, r).start()
        gat(1, r).wait_recv()
        gat(4, r).start()
        gat(6, r).start()

    def relay2(r):
        gat(3, r).wait_recv()
        gat(7, r).start()
        gat(4, r).wait_recv()
        gat(8, r).start()

    def rows_of(shard, off, n):
        return pl.ds(pl.multiple_of(shard * 128 + off, 16), n)

    near = (left, right, opp)
    xr_id = at_sp(z * 4 + (xx + 1) % 4)
    xl_id = at_sp(z * 4 + (xx + 3) % 4)
    x_left, x_right, x_opp = (xx + 3) % 4, (xx + 1) % 4, (xx + 2) % 4
    moves = {"m": (wo.at[:, rows_of(t, 0, 128), :], at_tp(mate))}
    for h in (0, 1):
        a_own = wo.at[0, rows_of(t, 64 * h, 64), :]
        moves["ar", h] = (a_own, at_tp(right))
        moves["al", h] = (a_own, at_tp(left))
        moves["afr", h] = (wo.at[0, rows_of(left, 64 * h, 32), :], at_tp(right))
        moves["afl", h] = (wo.at[0, rows_of(right, 64 * h + 32, 32), :], at_tp(left))
    for j in range(3):
        moves["am", j] = (wo.at[0, rows_of(near[j], 0, 128), :], at_tp(mate))
    b_own = wo.at[1, rows_of(t, 32 * xx, 32), :]
    moves["br"] = (b_own, at_tp(right))
    moves["bl"] = (b_own, at_tp(left))
    moves["bfr"] = (wo.at[1, rows_of(left, 32 * xx, 16), :], at_tp(right))
    moves["bfl"] = (wo.at[1, rows_of(right, 32 * xx + 16, 16), :], at_tp(left))
    for j in range(3):
        b_mine = wo.at[1, rows_of(near[j], 32 * xx, 32), :]
        moves["xr", j] = (b_mine, xr_id)
        moves["xl", j] = (b_mine, xl_id)
        moves["xfr", j] = (wo.at[1, rows_of(near[j], 32 * x_left, 16), :], xr_id)
        moves["xfl", j] = (wo.at[1, rows_of(near[j], 32 * x_right + 16, 16), :], xl_id)
        moves["xm", j] = (wo.at[1, rows_of(near[j], 0, 128), :], at_tp(mate))
    assert len(moves) == MOVES

    def move(*key):
        key = key if len(key) > 1 else key[0]
        ref, to = moves[key]
        k = list(moves).index(key)
        return send(ref, ref, os_.at[k], or_.at[k], to)

    xcopy.wait()
    own(0)
    own(1)

    pick = (lax.broadcasted_iota(jnp.int32, (8, 128), 0) == t).astype(BF)
    lane = lax.broadcasted_iota(jnp.int32, (8, 128), 1)
    w[:, 896:1024] = (
        mm(wb[...], jnp.where(lane < 64, pick, 0), TN)
        + mm(wd[...], jnp.where(lane < 64, 0, pick), TN)
    ).astype(BF)
    rate = jnp.exp(jnp.full((1, 128), dlog[t], F32))
    row, col = iotas((BLK, BLK))
    causal = row >= col
    strict = row > col
    tri = causal.astype(F32)
    mn[:, :128] = (row == col).astype(F32)
    mn[:, 128:] = jnp.zeros((BLK, BLK), F32)

    for cp in wcopies[:7]:
        cp.wait()

    def project(r):
        rows = pl.ds(pl.multiple_of(r * CHUNK, CHUNK), CHUNK)
        xr_ = xg[rows, :]
        xf = xr_.astype(F32)
        inv = lax.rsqrt(jnp.sum(xf * xf, axis=1, keepdims=True) / 2048.0 + NORM)
        raw = []
        for n in range(0, COLS, 256):
            d = jnp.dot(xr_, w[:, n : n + 256], preferred_element_type=F32) * inv
            raw += [d[:, :128], d[:, 128:]]
        q, k, v, dg, gv, gg, cg = [a.astype(BF).astype(F32) for a in raw[:7]]
        qs[rows, :] = unit_rows(q) * (128.0 ** -0.5)
        ks[rows, :] = unit_rows(k)
        vs[rows, :] = v
        dgs[rows, :] = dg * sigmoid(dg)
        cgs[rows, :] = cg * sigmoid(cg)
        turned = pltpu.roll(raw[7], 64, 1)
        low_lanes = lax.broadcasted_iota(jnp.int32, (CHUNK, 128), 1) < 64
        bes[rows, :] = sigmoid(jnp.where(low_lanes, raw[7], turned))
        lds[rows, :] = -rate * softplus(jnp.where(low_lanes, turned, raw[7]))
        below = pl.ds(pl.multiple_of(r * CHUNK + 32, 32), CHUNK)
        pad[below, :] = (gv * sigmoid(gg)).astype(BF).astype(F32)

    def delta(r):
        spans = [pl.ds(pl.multiple_of(r * GROUP + b * BLK, BLK), BLK) for b in range(PER)]
        sums, lows, scores = [], [], []
        for rows in spans:
            total = lax.dot_general(
                tri, lds[rows, :], (NN, ((), ())),
                precision=lax.Precision.HIGHEST, preferred_element_type=F32,
            )
            spread = total - total.T
            damp = jnp.where(causal, jnp.exp(jnp.where(causal, spread, 0.0)), 0.0)
            kb = ks[rows, :].astype(BF)
            both = mm(jnp.concatenate([kb, qs[rows, :].astype(BF)], axis=0), kb, NT)
            lows.append(jnp.where(strict, both[:BLK] * bes[rows, :] * damp, 0.0))
            scores.append(both[BLK:] * damp)
            sums.append(total)
        inverses = block_inverse(lows)
        later = []
        for rows, total, score, inv in zip(spans, sums, scores, inverses):
            grow = jnp.exp(total)
            kv, be = ks[rows, :], bes[rows, :]
            rhs = jnp.concatenate([vs[rows, :] * be, kv * be * grow], axis=1)
            solved = mm(inv, rhs).astype(BF)
            mixed = mm(score, solved)
            tail = total[BLK - 1 : BLK, :]
            fresh = mm(kv * jnp.exp(tail - total), solved, TN)
            later.append(
                (
                    jnp.concatenate([qs[rows, :] * grow - mixed[:, 128:], fresh[:, 128:]], axis=0),
                    mixed[:, :128], fresh[:, :128], jnp.exp(tail),
                )
            )
        state = mn[...]
        for rows, (lhs, o_here, n_here, fade) in zip(spans, later):
            moved = mm(lhs, state)
            qcs[rows, :] = moved[:BLK, :128]
            ocs[rows, :] = moved[:BLK, 128:] + o_here
            m_next = state[:, :128] * fade - moved[BLK:, :128]
            n_next = state[:, 128:] * fade - moved[BLK:, 128:] + n_here
            state = jnp.concatenate([m_next, n_next], axis=1)
        mn[...] = state

    def arrive(r):
        for kind in (2, 5, 6, 7, 8):
            gat(kind, r).wait_recv()

    relay1(0)
    own(2)
    relay1(1)
    own(3)
    relay2(0)
    for kk in (7, 8):
        wcopies[kk].wait()

    @pl.loop(0, 2)
    def _(p):
        arrive(2 * p)
        project(2 * p)

        @pl.when(p == 0)
        def _():
            relay1(2)
            relay2(1)

        arrive(2 * p + 1)
        project(2 * p + 1)

        @pl.when(p == 0)
        def _():
            relay1(3)

        delta(p)

        @pl.when(p == 0)
        def _():
            relay2(2)
            relay2(3)
            for key in ("br", "bl", "m"):
                move(key).start()
            move("ar", 0).start()
            move("al", 0).start()

    own_x = mn[...].astype(BF)
    mnx[xx] = own_x

    def xsend(d):
        return send(mnx.at[xx], mnx.at[xx], xs.at[d - 1], xr.at[d - 1],
                    at_sp(z * 4 + (xx + d) % 4))

    for d in (1, 2, 3):
        xsend(d).start()
    halo_s[...] = pad[ROWS : ROWS + 32, :].astype(BF)
    hcopy = send(halo_s, halo_r, hs, hr, at_sp((sp + 1) % 32))
    hcopy.start()
    move("br").wait_recv()
    move("bfr").start()
    move("bl").wait_recv()
    move("bfl").start()
    move("ar", 1).start()
    move("al", 1).start()
    for j in (0, 1):
        move("xr", j).start()
        move("xl", j).start()

    tapf = taps[...].astype(F32)

    def conv_rows(i):
        acc = jnp.zeros((64, 128), F32)
        for j in range(TAPS):
            acc = acc + pad[pl.ds(i * 64 + 2 + j, 64), :] * tapf[j : j + 1, :]
        filt[pl.ds(pl.multiple_of(i * 64, 64), 64), :] = acc

    @pl.loop(1, ROWS // 64)
    def _(i):
        conv_rows(i)

    hcopy.wait_recv()
    keep = (sp > 0).astype(F32)
    pad[0:32, :] = halo_r[...].astype(F32) * keep
    conv_rows(0)
    for b in range(ROWS // BLK):
        lanes = slice(b * BLK, (b + 1) * BLK)
        ft = filt[lanes, :].T
        sts[0:1, lanes] = jnp.sum(ft, axis=0, keepdims=True)
        sts[1:2, lanes] = jnp.sum(ft * ft, axis=0, keepdims=True)

    def ssend(d):
        return send(sts, str_.at[t], ss.at[d - 1], sr.at[d - 1], at_tp((t + d) % 8))

    for d in range(1, 8):
        ssend(d).start()
    str_[t] = sts[...]

    def chain(slots, mine):
        total = slots[0].astype(F32)
        m_in = jnp.where(mine > 0, total[:, :128], (row == col).astype(F32))
        n_in = jnp.where(mine > 0, total[:, 128:], 0.0)
        for k in (1, 2, 3):
            piece = slots[k]
            moved = mm(piece[:, :128], total)
            total = jnp.concatenate(
                [moved[:, :128], moved[:, 128:] + piece[:, 128:].astype(F32)], axis=1
            )
            if k < 3:
                m_in = jnp.where(mine > k, total[:, :128], m_in)
                n_in = jnp.where(mine > k, total[:, 128:], n_in)
        return m_in, n_in, total

    for d in (1, 2, 3):
        xsend(d).wait_recv()
    mxp, nxp, xtotal = chain(mnx, xx)
    mnz[zi] = xtotal.astype(BF)

    def zsend(d):
        return send(mnz.at[zi], mnz.at[zi], zs.at[d - 1], zr.at[d - 1],
                    at_sp((zq * 4 + (zi + d) % 4) * 4 + xx))

    for d in (1, 2, 3):
        zsend(d).start()

    move("bfr").wait_recv()
    move("bfl").wait_recv()
    move("xr", 2).start()
    move("xl", 2).start()
    move("ar", 0).wait_recv()
    move("afr", 0).start()
    move("al", 0).wait_recv()
    move("afl", 0).start()

    for d in range(1, 8):
        ssend(d).wait_recv()
    both = str_[0]
    for k in range(1, 8):
        both = both + str_[k]
    center = both[0:1, :] / 1024.0
    variance = jnp.maximum(both[1:2, :] / 1024.0 - center * center, 0.0)
    scale = lax.rsqrt(variance + VAR)
    for b in range(ROWS // BLK):
        lanes = slice(b * BLK, (b + 1) * BLK)
        cen = jnp.broadcast_to(center[:, lanes], (BLK, BLK)).T
        sca = jnp.broadcast_to(scale[:, lanes], (BLK, BLK)).T
        normed = (filt[lanes, :] - cen) * sca * lng[...] + lns[...]
        cms[lanes, :] = (normed * sigmoid(normed) * cgs[lanes, :]).astype(BF)

    def a2a(src, dst, s_sem, r_sem, d):
        to = (t + d) % 8
        rows = pl.ds(pl.multiple_of(to * BLK, BLK), BLK)
        return send(src.at[rows, :], dst.at[t], s_sem.at[d - 1], r_sem.at[d - 1], at_tp(to))

    for d in range(1, 8):
        a2a(cms, cmr, cs, cr, d).start()
    cmr[t] = cms[own_rows, :]

    for d in (1, 2, 3):
        zsend(d).wait_recv()
    mzp, nzp, ztotal = chain(mnz, zi)
    s4s[...] = ztotal[:, 128:].astype(BF)
    fcopy = send(s4s, s4r, fs, fr, at_sp(((z + 4) % 8) * 4 + xx))
    fcopy.start()
    moved = mm(mxp, jnp.concatenate([mzp, nzp], axis=1))
    mpre, npre = moved[:, :128], moved[:, 128:] + nxp
    for j in (0, 1, 2):
        move("xr", j).wait_recv()
        move("xfr", j).start()
        move("xl", j).wait_recv()
        move("xfl", j).start()
    move("ar", 1).wait_recv()
    move("afr", 1).start()
    move("am", 0).start()
    move("al", 1).wait_recv()
    move("afl", 1).start()
    move("am", 1).start()
    fcopy.wait_recv()
    begin = s4r[...].astype(F32) * (zq > 0).astype(F32)
    carried = mm(mpre, begin) + npre

    for b in range(ROWS // BLK):
        lanes = slice(b * BLK, (b + 1) * BLK)
        o = ocs[lanes, :] + mm(qcs[lanes, :], carried)
        o = o * lax.rsqrt(jnp.mean(o * o, axis=-1, keepdims=True) + NORM) * hgain[...]
        dms[lanes, :] = (o * dgs[lanes, :]).astype(BF)
    for d in range(1, 8):
        a2a(dms, dmr, ds_, dr, d).start()
    dmr[t] = dms[own_rows, :]

    for j in (0, 1, 2):
        move("xfr", j).wait_recv()
        move("xfl", j).wait_recv()
        move("xm", j).start()
    for h in (0, 1):
        move("afr", h).wait_recv()
        move("afl", h).wait_recv()
    move("am", 2).start()
    for d in range(1, 8):
        a2a(cms, cmr, cs, cr, d).wait_recv()
    move("m").wait_recv()
    for j in (0, 1, 2):
        move("xm", j).wait_recv()
        move("am", j).wait_recv()
    for d in range(1, 8):
        a2a(dms, dmr, ds_, dr, d).wait_recv()

    lhs_d = jnp.concatenate([dmr[k] for k in range(8)], axis=1)
    lhs_c = jnp.concatenate([cmr[k] for k in range(8)], axis=1)

    def ocopy(n):
        lanes = pl.ds(pl.multiple_of(n * 256, 256), 256)
        return pltpu.make_async_copy(stage.at[n], out.at[:, lanes], osem.at[n])

    @pl.loop(0, 8)
    def _(n):
        lanes = pl.ds(pl.multiple_of(n * 256, 256), 256)
        acc = jnp.dot(lhs_d, wo[0, :, lanes], preferred_element_type=F32)
        acc = acc + jnp.dot(lhs_c, wo[1, :, lanes], preferred_element_type=F32)
        stage[n] = acc.astype(BF)
        ocopy(n).start()

    for n in range(8):
        ocopy(n).wait()
    for r in range(CHUNKS):
        for kind in range(9):
            gat(kind, r).wait_send()
    for key in moves:
        move(*(key if isinstance(key, tuple) else (key,))).wait_send()
    for d in (1, 2, 3):
        xsend(d).wait_send()
        zsend(d).wait_send()
    hcopy.wait_send()
    fcopy.wait_send()
    for d in range(1, 8):
        ssend(d).wait_send()
        a2a(cms, cmr, cs, cr, d).wait_send()
        a2a(dms, dmr, ds_, dr, d).wait_send()


def local(*args):
    (tokens, w_query, w_key, w_value, w_delta_gate, w_glu_value, w_glu_gate, w_conv_gate,
     w_beta, w_decay, decay_log, head_gain, conv_taps, ln_gain, ln_shift, out_delta,
     out_conv) = args
    vm = pl.BlockSpec(memory_space=pltpu.VMEM)
    hb = pl.BlockSpec(memory_space=pl.ANY)
    sm = pl.BlockSpec(memory_space=pltpu.SMEM)
    big = lambda kind: pltpu.VMEM((ROWS, 128), kind)
    dma = pltpu.SemaphoreType.DMA
    return pl.pallas_call(
        kernel,
        out_shape=jax.ShapeDtypeStruct((BLK, 2048), BF),
        in_specs=[hb] * 8 + [vm, vm, sm] + [vm] * 4 + [hb, hb],
        out_specs=hb,
        scratch_shapes=[
            pltpu.VMEM((ROWS, 2048), BF),
            pltpu.VMEM((2048, COLS), BF),
            pltpu.VMEM((2, 1024, 2048), BF),
            big(F32), big(F32), big(F32), big(F32), big(F32), big(F32), big(F32),
            pltpu.VMEM((ROWS + 32, 128), F32),
            big(F32), big(F32), big(F32),
            pltpu.VMEM((BLK, 256), F32),
            pltpu.VMEM((4, BLK, 256), BF),
            pltpu.VMEM((4, BLK, 256), BF),
            pltpu.VMEM((BLK, BLK), BF),
            pltpu.VMEM((BLK, BLK), BF),
            pltpu.VMEM((32, 128), BF),
            pltpu.VMEM((32, 128), BF),
            pltpu.VMEM((2, ROWS), F32),
            pltpu.VMEM((8, 2, ROWS), F32),
            big(BF), big(BF),
            pltpu.VMEM((8, BLK, BLK), BF),
            pltpu.VMEM((8, BLK, BLK), BF),
            pltpu.VMEM((8, BLK, 256), BF),
            dma((10,)),
            dma((9, CHUNKS)), dma((9, CHUNKS)),
            dma((MOVES,)), dma((MOVES,)),
            dma((3,)), dma((3,)), dma((3,)), dma((3,)),
            dma, dma, dma, dma,
            dma((7,)), dma((7,)), dma((7,)), dma((7,)), dma((7,)), dma((7,)), dma((8,)),
        ],
        compiler_params=pltpu.CompilerParams(
            collective_id=0, has_side_effects=True, vmem_limit_bytes=60 * 1024 * 1024
        ),
        name="layer",
    )(
        tokens, w_query, w_key, w_value, w_delta_gate, w_glu_value, w_glu_gate, w_conv_gate,
        w_beta.T, w_decay.T, decay_log, head_gain.reshape(1, 128), conv_taps,
        ln_gain.reshape(1, 128), ln_shift.reshape(1, 128), out_delta, out_conv,
    )


def solution(mesh):
    cut = P(None, "tp")
    placed = (P("sp", "tp"),) + (cut,) * 7 + (P(),) * 4 + (
        cut, P("tp"), P("tp"), P("tp", None), P("tp", None),
    )
    return jax.shard_map(
        local, mesh=mesh, in_specs=placed, out_specs=P(("sp", "tp"), None), check_vma=False
    )
```

```python
import jax
import jax.numpy as jnp
from jax import lax
from jax.experimental import pallas as pl
from jax.experimental.pallas import tpu as pltpu
from jax.sharding import PartitionSpec as P

BF = jnp.bfloat16
F32 = jnp.float32
ROWS = 1024
SHARD = 256
BLK = 128
CHUNK = 256
CHUNKS = ROWS // CHUNK
HALF = CHUNK // 2
COLS = 8 * 128
SEMS = (
    ("w", "wo", "x", "out", "gs", "ms", "xs", "zs", "fs", "hs", "ss", "ds", "cs")
    + tuple(f"g{k}{r}" for k in range(3) for r in range(CHUNKS))
    + ("a", "af", "by", "bf", "b0", "b1", "bx", "bm", "zy", "zf", "z0", "zx", "zm")
    + ("xr", "zr", "fr", "hr", "sr", "dr", "cr")
)
TAPS = 31
FAR_FIRST = (4, 5, 3, 2, 6, 1, 7)
NORM = 1e-06
VAR = 1e-05
NN = ((1,), (0,))
NT = ((1,), (1,))
TN = ((0,), (0,))


def mm(a, b, dims=NN):
    return lax.dot_general(
        a.astype(BF), b.astype(BF), (dims, ((), ())), preferred_element_type=F32
    )


def iotas(shape):
    return lax.broadcasted_iota(jnp.int32, shape, 0), lax.broadcasted_iota(jnp.int32, shape, 1)


def softplus(v):
    return jnp.maximum(v, 0.0) + jnp.log1p(jnp.exp(-jnp.abs(v)))


def sigmoid(v):
    return jax.nn.sigmoid(v)


def unit_rows(v):
    return v * lax.rsqrt(jnp.sum(v * v, axis=-1, keepdims=True) + NORM)


def block_inverse(lows):
    row, col = iotas((BLK, BLK))
    eye = (row == col).astype(F32)
    parts = [eye - jnp.where((row // 2 == col // 2), low, 0.0) for low in lows]
    m = 2
    while m < BLK:
        pick = (row // (2 * m) == col // (2 * m)) & (row // m != col // m)
        packed = [p.astype(BF) for p in parts]
        inner = [mm(jnp.where(pick, low, 0.0), p) for low, p in zip(lows, packed)]
        parts = [t - mm(p, i) for t, p, i in zip(parts, packed, inner)]
        m *= 2
    return parts


def kernel(
    x, wq, wk, wv, wdg, wgv, wgg, wcg, wb, wd, dlog, hgain, taps, lng, lns, od, oc,
    out,
    xg, w, wo, qs, ks, vs, dgs, cgs, bes, lds, pad, filt, qcs, ocs, mn, mnx, mnz, s4s, s4r,
    halo_s, halo_r, sts, str_, dms, cms, dmr, cmr, stage, half,
    sems,
):
    sp = lax.axis_index("sp")
    t = lax.axis_index("tp")
    y, c = t // 2, t % 2
    z, xx = sp // 4, sp % 4
    zq, zi = z // 4, z % 4
    right = ((y + 1) % 4) * 2 + c
    left = ((y + 3) % 4) * 2 + c
    opp = ((y + 2) % 4) * 2 + c
    mate = y * 2 + (1 - c)

    def at_tp(k):
        return {"sp": sp, "tp": k}

    def at_sp(k):
        return {"sp": k, "tp": t}

    def sem(name):
        return sems.at[SEMS.index(name)]

    def await_bytes(ref, name):
        pltpu.make_async_copy(ref, ref, sem(name)).wait()

    wrefs = (wq, wk, wv, wdg, wgv, wgg, wcg)
    wcopies = [
        pltpu.make_async_copy(ref, w.at[:, k * 128 : (k + 1) * 128], sem("w"))
        for k, ref in enumerate(wrefs)
    ]
    own_rows = pl.ds(pl.multiple_of(t * 128, 128), 128)
    wcopies.append(pltpu.make_async_copy(od, wo.at[0, own_rows, :], sem("wo")))
    wcopies.append(pltpu.make_async_copy(oc, wo.at[1, own_rows, :], sem("wo")))

    def cols_of(k):
        return pl.ds(pl.multiple_of(k * SHARD, SHARD), SHARD)

    xcopy = pltpu.make_async_copy(x, xg.at[:, cols_of(t)], sem("x"))
    xcopy.start()
    for cp in wcopies:
        cp.start()

    bar = pltpu.get_barrier_semaphore()
    peers = [at_tp((t + d) % 8) for d in range(1, 8)]
    peers += [at_sp(z * 4 + (xx + d) % 4) for d in range(1, 4)]
    peers += [at_sp((zq * 4 + (zi + d) % 4) * 4 + xx) for d in range(1, 4)]
    peers += [at_sp((7 - z) * 4 + xx), at_sp((sp + 1) % 32), at_sp((sp + 31) % 32)]
    for peer in peers:
        pl.semaphore_signal(bar, inc=1, device_id=peer, device_id_type=pl.DeviceIdType.MESH)
    pl.semaphore_wait(bar, len(peers))

    def send(src, dst, ssem, rsem, to):
        return pltpu.make_async_remote_copy(
            src_ref=src, dst_ref=dst, send_sem=ssem, recv_sem=rsem,
            device_id=to, device_id_type=pl.DeviceIdType.MESH,
        )

    def gat(kind, r):
        base = r * CHUNK
        whole = pl.ds(pl.multiple_of(base, CHUNK), CHUNK)
        first = pl.ds(pl.multiple_of(base, HALF), HALF)
        second = pl.ds(pl.multiple_of(base + HALF, HALF), HALF)
        rows = (whole, whole, whole, first, second, whole, whole, first, second)[kind]
        shard = (t, t, t, left, right, left, right, opp, opp)[kind]
        to = (right, left, mate, right, left, mate, mate, mate, mate)[kind]
        dst = xg.at[rows, cols_of(shard)]
        return send(dst, dst, sem("gs"), sem(f"g{(0, 0, 2, 1, 1, 2, 2, 2, 2)[kind]}{r}"), at_tp(to))

    def own(r):
        for kind in (0, 1, 2):
            gat(kind, r).start()

    def relay1(r):
        await_bytes(xg.at[0:CHUNK, 0:512], f"g0{r}")
        for kind in (3, 4, 5, 6):
            gat(kind, r).start()

    def relay2(r):
        await_bytes(xg.at[0:CHUNK, 0:256], f"g1{r}")
        gat(7, r).start()
        gat(8, r).start()

    def rows_of(shard, off, n):
        return pl.ds(pl.multiple_of(shard * 128 + off, 8), n)

    near = (left, right, opp)
    xr_id = at_sp(z * 4 + (xx + 1) % 4)
    xl_id = at_sp(z * 4 + (xx + 3) % 4)
    zr_id = at_sp(((z + 1) % 8) * 4 + xx)
    zl_id = at_sp(((z + 7) % 8) * 4 + xx)
    moves = {"m": (wo.at[:, rows_of(t, 0, 128), :], at_tp(mate))}
    a_own = wo.at[0, rows_of(t, 0, 64), :]
    moves["ar"] = (a_own, at_tp(right))
    moves["al"] = (a_own, at_tp(left))
    moves["afr"] = (wo.at[0, rows_of(left, 0, 32), :], at_tp(right))
    moves["afl"] = (wo.at[0, rows_of(right, 32, 32), :], at_tp(left))
    for j in range(3):
        moves["am", j] = (wo.at[0, rows_of(near[j], 0, 64), :], at_tp(mate))

    def spread_moves(name, w_at, base, piece, place, to_right, to_left):
        def part(shard, off, n):
            return wo.at[w_at, rows_of(shard, base + off, n), :]

        half = piece // 2
        mine = piece * place
        before, after = piece * ((place + 3) % 4), piece * ((place + 1) % 4)
        moves[name, "yr"] = (part(t, mine, piece), at_tp(right))
        moves[name, "yl"] = (part(t, mine, piece), at_tp(left))
        moves[name, "yfr"] = (part(left, mine, half), at_tp(right))
        moves[name, "yfl"] = (part(right, mine + half, half), at_tp(left))
        for j in range(3):
            shard = near[j]
            moves[name, "r", j] = (part(shard, mine, piece), to_right)
            moves[name, "l", j] = (part(shard, mine, piece), to_left)
            moves[name, "fr", j] = (part(shard, before, half), to_right)
            moves[name, "fl", j] = (part(shard, after + half, half), to_left)
            across = piece * ((place + 2) % 4)
            for k, off in enumerate((mine, before, after, across)):
                moves[name, f"m{k}", j] = (part(shard, off, piece), at_tp(mate))

    spread_moves("b", 1, 0, 32, xx, xr_id, xl_id)
    spread_moves("z", 0, 64, 16, zi, zr_id, zl_id)

    def go(name, *tags):
        for tag in tags:
            for key in [k for k in moves if k[:2] == (name, tag)]:
                move(*key).start()

    def landing(key):
        if key == "m":
            return "bm"
        if isinstance(key, str):
            return "a" if key in ("ar", "al") else "af"
        name, tag = key[:2]
        if name == "am":
            return "zm"
        if tag in ("yr", "yl"):
            return name + "y"
        if tag in ("yfr", "yfl"):
            return name + "f"
        if tag in ("r", "l"):
            return name + ("1" if name == "b" and key[2] > 0 else "0")
        return name + ("x" if tag in ("fr", "fl") else "m")

    def move(*key):
        key = key if len(key) > 1 else key[0]
        ref, to = moves[key]
        return send(ref, ref, sem("ms"), sem(landing(key)), to)

    def got(name, rows):
        await_bytes(wo.at[0, 0:rows, :], name)

    xcopy.wait()
    own(0)
    own(1)

    pick = (lax.broadcasted_iota(jnp.int32, (8, 128), 0) == t).astype(BF)
    lane = lax.broadcasted_iota(jnp.int32, (8, 128), 1)
    w[:, 896:1024] = (
        mm(wb[...], jnp.where(lane < 64, pick, 0), TN)
        + mm(wd[...], jnp.where(lane < 64, 0, pick), TN)
    ).astype(BF)
    rate = jnp.exp(jnp.full((1, 128), dlog[t], F32))
    row, col = iotas((BLK, BLK))
    causal = row >= col
    strict = row > col
    tri = causal.astype(F32)
    mn[:, :128] = (row == col).astype(F32)
    mn[:, 128:] = jnp.zeros((BLK, BLK), F32)

    await_bytes(w.at[:, :896], "w")

    def project(r):
        rows = slice(r * CHUNK, (r + 1) * CHUNK)
        xr_ = xg[rows, :]
        xf = xr_.astype(F32)
        inv = lax.rsqrt(jnp.sum(xf * xf, axis=1, keepdims=True) / 2048.0 + NORM)
        raw = []
        for n in range(0, COLS, 256):
            d = jnp.dot(xr_, w[:, n : n + 256], preferred_element_type=F32) * inv
            raw += [d[:, :128], d[:, 128:]]
        q, k, v, dg, gv, gg, cg = [a.astype(BF).astype(F32) for a in raw[:7]]
        qs[rows, :] = unit_rows(q) * (128.0 ** -0.5)
        ks[rows, :] = unit_rows(k)
        vs[rows, :] = v
        dgs[rows, :] = dg * sigmoid(dg)
        cgs[rows, :] = cg * sigmoid(cg)
        turned = pltpu.roll(raw[7], 64, 1)
        low_lanes = lax.broadcasted_iota(jnp.int32, (CHUNK, 128), 1) < 64
        bes[rows, :] = sigmoid(jnp.where(low_lanes, raw[7], turned))
        lds[rows, :] = -rate * softplus(jnp.where(low_lanes, turned, raw[7]))
        below = slice(r * CHUNK + 32, (r + 1) * CHUNK + 32)
        pad[below, :] = (gv * sigmoid(gg)).astype(BF).astype(F32)

    def delta(first, last, mid=None):
        spans = [slice(b * BLK, (b + 1) * BLK) for b in range(first, last)]
        sums, lows, scores = [], [], []
        for rows in spans:
            total = lax.dot_general(
                tri, lds[rows, :], (NN, ((), ())),
                precision=lax.Precision.HIGHEST, preferred_element_type=F32,
            )
            spread = total - total.T
            damp = jnp.where(causal, jnp.exp(jnp.where(causal, spread, 0.0)), 0.0)
            kb = ks[rows, :].astype(BF)
            both = mm(jnp.concatenate([kb, qs[rows, :].astype(BF)], axis=0), kb, NT)
            lows.append(jnp.where(strict, both[:BLK] * bes[rows, :] * damp, 0.0))
            scores.append(both[BLK:] * damp)
            sums.append(total)
        inverses = block_inverse(lows)
        if mid is not None:
            mid()
        later = []
        for rows, total, score, inv in zip(spans, sums, scores, inverses):
            grow = jnp.exp(total)
            kv, be = ks[rows, :], bes[rows, :]
            rhs = jnp.concatenate([vs[rows, :] * be, kv * be * grow], axis=1)
            solved = mm(inv, rhs).astype(BF)
            mixed = mm(score, solved)
            tail = total[BLK - 1 : BLK, :]
            fresh = mm(kv * jnp.exp(tail - total), solved, TN)
            later.append(
                (
                    jnp.concatenate([qs[rows, :] * grow - mixed[:, 128:], fresh[:, 128:]], axis=0),
                    mixed[:, :128], fresh[:, :128], jnp.exp(tail),
                )
            )
        state = mn[...]
        for rows, (lhs, o_here, n_here, fade) in zip(spans, later):
            moved = mm(lhs, state)
            qcs[rows, :] = moved[:BLK, :128]
            ocs[rows, :] = moved[:BLK, 128:] + o_here
            m_next = state[:, :128] * fade - moved[BLK:, :128]
            n_next = state[:, 128:] * fade - moved[BLK:, 128:] + n_here
            state = jnp.concatenate([m_next, n_next], axis=1)
        mn[...] = state

    def arrive(r):
        await_bytes(xg.at[0:CHUNK, 0:1024], f"g2{r}")

    relay1(0)
    own(2)
    relay1(1)
    own(3)
    relay2(0)
    await_bytes(wo.at[:, 0:128, :], "wo")

    arrive(0)
    project(0)
    relay1(2)
    delta(0, 2, lambda: relay2(1))
    relay1(3)
    arrive(1)
    project(1)

    def middle():
        relay2(2)
        go("b", "yr", "yl")
        go("z", "yr", "yl")

    delta(2, 4, middle)
    relay2(3)
    move("m").start()
    arrive(2)
    project(2)
    arrive(3)
    project(3)
    delta(4, 8)
    own_x = mn[...].astype(BF)
    mnx[xx] = own_x

    def xsend(d):
        return send(mnx.at[xx], mnx.at[xx], sem("xs"), sem("xr"),
                    at_sp(z * 4 + (xx + d) % 4))

    for d in (1, 2, 3):
        xsend(d).start()
    halo_s[...] = pad[ROWS : ROWS + 32, :].astype(BF)
    hcopy = send(halo_s, halo_r, sem("hs"), sem("hr"), at_sp((sp + 1) % 32))
    hcopy.start()
    for name, rows in (("b", 64), ("z", 32)):
        got(name + "y", rows)
        go(name, "yfr", "yfl")
        for j in (0, 1):
            move(name, "r", j).start()
            move(name, "l", j).start()
            move(name, "m0", j).start()
    move("ar").start()
    move("al").start()

    tapf = taps[...].astype(F32)

    def conv_rows(i):
        acc = jnp.zeros((64, 128), F32)
        for j in range(TAPS):
            acc = acc + pad[pl.ds(i * 64 + 2 + j, 64), :] * tapf[j : j + 1, :]
        filt[pl.ds(pl.multiple_of(i * 64, 64), 64), :] = acc

    @pl.loop(1, ROWS // 64)
    def _(i):
        conv_rows(i)

    hcopy.wait_recv()
    keep = (sp > 0).astype(F32)
    pad[0:32, :] = halo_r[...].astype(F32) * keep
    conv_rows(0)
    for b in range(ROWS // BLK):
        lanes = slice(b * BLK, (b + 1) * BLK)
        ft = filt[lanes, :].T
        sts[0:1, lanes] = jnp.sum(ft, axis=0, keepdims=True)
        sts[1:2, lanes] = jnp.sum(ft * ft, axis=0, keepdims=True)

    def ssend(d):
        return send(sts, str_.at[t], sem("ss"), sem("sr"), at_tp((t + d) % 8))

    for d in range(1, 8):
        ssend(d).start()
    str_[t] = sts[...]

    def chain(slots, mine):
        total = slots[0].astype(F32)
        m_in = jnp.where(mine > 0, total[:, :128], (row == col).astype(F32))
        n_in = jnp.where(mine > 0, total[:, 128:], 0.0)
        for k in (1, 2, 3):
            piece = slots[k]
            moved = mm(piece[:, :128], total)
            total = jnp.concatenate(
                [moved[:, :128], moved[:, 128:] + piece[:, 128:].astype(F32)], axis=1
            )
            if k < 3:
                m_in = jnp.where(mine > k, total[:, :128], m_in)
                n_in = jnp.where(mine > k, total[:, 128:], n_in)
        return m_in, n_in, total

    await_bytes(mnx.at[0:3], "xr")
    mxp, nxp, xtotal = chain(mnx, xx)
    mnz[zi] = xtotal.astype(BF)

    def zsend(d):
        return send(mnz.at[zi], mnz.at[zi], sem("zs"), sem("zr"),
                    at_sp((zq * 4 + (zi + d) % 4) * 4 + xx))

    for d in (1, 2, 3):
        zsend(d).start()

    got("bf", 32)
    got("zf", 16)
    for name in ("b", "z"):
        for tag in ("r", "l", "m0"):
            move(name, tag, 2).start()
    got("b0", 64)
    for tag in ("fr", "fl", "m1", "m2"):
        move("b", tag, 0).start()
    await_bytes(str_.at[0:7], "sr")
    both = str_[0]
    for k in range(1, 8):
        both = both + str_[k]
    center = both[0:1, :] / 1024.0
    variance = jnp.maximum(both[1:2, :] / 1024.0 - center * center, 0.0)
    scale = lax.rsqrt(variance + VAR)
    for b in range(ROWS // BLK):
        lanes = slice(b * BLK, (b + 1) * BLK)
        cen = jnp.broadcast_to(center[:, lanes], (BLK, BLK)).T
        sca = jnp.broadcast_to(scale[:, lanes], (BLK, BLK)).T
        normed = (filt[lanes, :] - cen) * sca * lng[...] + lns[...]
        cms[lanes, :] = (normed * sigmoid(normed) * cgs[lanes, :]).astype(BF)

    def a2a(src, dst, s_sem, r_sem, d):
        to = (t + d) % 8
        rows = pl.ds(pl.multiple_of(to * BLK, BLK), BLK)
        return send(src.at[rows, :], dst.at[t], sem(s_sem), sem(r_sem), at_tp(to))

    for d in FAR_FIRST:
        a2a(cms, cmr, "cs", "cr", d).start()
    cmr[t] = cms[own_rows, :]
    got("a", 128)
    for key in ("afr", "afl"):
        move(key).start()
    move("am", 0).start()
    move("am", 1).start()

    await_bytes(mnz.at[0:3], "zr")
    mzp, nzp, ztotal = chain(mnz, zi)
    s4s[...] = ztotal[:, 128:].astype(BF)
    fcopy = send(s4s, s4r, sem("fs"), sem("fr"), at_sp((7 - z) * 4 + xx))
    fcopy.start()
    moved = mm(mxp, jnp.concatenate([mzp, nzp], axis=1))
    mpre, npre = moved[:, :128], moved[:, 128:] + nxp
    got("b1", 128)
    for j in (1, 2):
        for tag in ("fr", "fl", "m1", "m2"):
            move("b", tag, j).start()
    got("z0", 96)
    go("z", "fr", "fl", "m1", "m2")
    fcopy.wait_recv()
    begin = s4r[...].astype(F32) * (zq > 0).astype(F32)
    carried = mm(mpre, begin) + npre

    for i, d in enumerate(FAR_FIRST + (0,)):
        lanes = pl.ds(pl.multiple_of(lax.rem(t + d, 8) * BLK, BLK), BLK)
        o = ocs[lanes, :] + mm(qcs[lanes, :], carried)
        o = o * lax.rsqrt(jnp.mean(o * o, axis=-1, keepdims=True) + NORM) * hgain[...]
        dms[lanes, :] = (o * dgs[lanes, :]).astype(BF)
        if i in (3, 7):
            for e in FAR_FIRST[max(i - 4, 0) : i]:
                a2a(dms, dmr, "ds", "dr", e).start()
    dmr[t] = dms[own_rows, :]

    got("bx", 96)
    go("b", "m3")
    got("zx", 48)
    go("z", "m3")
    got("af", 64)
    move("am", 2).start()
    await_bytes(cmr.at[0:7], "cr")
    got("bm", 640)
    lhs_c = jnp.concatenate([cmr[k] for k in range(8)], axis=1)

    @pl.loop(0, 8)
    def _(n):
        lanes = pl.ds(pl.multiple_of(n * 256, 256), 256)
        half[n] = jnp.dot(lhs_c, wo[1, :, lanes], preferred_element_type=F32)

    got("zm", 384)
    await_bytes(dmr.at[0:7], "dr")

    lhs_d = jnp.concatenate([dmr[k] for k in range(8)], axis=1)

    def ocopy(n):
        lanes = pl.ds(pl.multiple_of(n * 256, 256), 256)
        return pltpu.make_async_copy(stage.at[n], out.at[:, lanes], sem("out"))

    @pl.loop(0, 8)
    def _(n):
        lanes = pl.ds(pl.multiple_of(n * 256, 256), 256)
        acc = jnp.dot(lhs_d, wo[0, :, lanes], preferred_element_type=F32)
        stage[n] = (acc + half[n]).astype(BF)
        ocopy(n).start()

    await_bytes(stage, "out")
    await_bytes(xg.at[0:896, :], "gs")
    await_bytes(wo.at[:, 0:896, :], "ms")
    await_bytes(mnx.at[0:3], "xs")
    await_bytes(mnz.at[0:3], "zs")
    await_bytes(s4s, "fs")
    await_bytes(halo_s, "hs")
    await_bytes(str_.at[0:7], "ss")
    await_bytes(dmr.at[0:7], "ds")
    await_bytes(cmr.at[0:7], "cs")


def local(*args):
    (tokens, w_query, w_key, w_value, w_delta_gate, w_glu_value, w_glu_gate, w_conv_gate,
     w_beta, w_decay, decay_log, head_gain, conv_taps, ln_gain, ln_shift, out_delta,
     out_conv) = args
    vm = pl.BlockSpec(memory_space=pltpu.VMEM)
    hb = pl.BlockSpec(memory_space=pl.ANY)
    sm = pl.BlockSpec(memory_space=pltpu.SMEM)
    big = lambda kind: pltpu.VMEM((ROWS, 128), kind)
    dma = pltpu.SemaphoreType.DMA
    return pl.pallas_call(
        kernel,
        out_shape=jax.ShapeDtypeStruct((BLK, 2048), BF),
        in_specs=[hb] * 8 + [vm, vm, sm] + [vm] * 4 + [hb, hb],
        out_specs=hb,
        scratch_shapes=[
            pltpu.VMEM((ROWS, 2048), BF),
            pltpu.VMEM((2048, COLS), BF),
            pltpu.VMEM((2, 1024, 2048), BF),
            big(F32), big(F32), big(F32), big(F32), big(F32), big(F32), big(F32),
            pltpu.VMEM((ROWS + 32, 128), F32),
            big(F32), big(F32), big(F32),
            pltpu.VMEM((BLK, 256), F32),
            pltpu.VMEM((4, BLK, 256), BF),
            pltpu.VMEM((4, BLK, 256), BF),
            pltpu.VMEM((BLK, BLK), BF),
            pltpu.VMEM((BLK, BLK), BF),
            pltpu.VMEM((32, 128), BF),
            pltpu.VMEM((32, 128), BF),
            pltpu.VMEM((2, ROWS), F32),
            pltpu.VMEM((8, 2, ROWS), F32),
            big(BF), big(BF),
            pltpu.VMEM((8, BLK, BLK), BF),
            pltpu.VMEM((8, BLK, BLK), BF),
            pltpu.VMEM((8, BLK, 256), BF),
            pltpu.VMEM((8, BLK, 256), F32),
            dma((len(SEMS),)),
        ],
        compiler_params=pltpu.CompilerParams(
            collective_id=0, has_side_effects=True, vmem_limit_bytes=60 * 1024 * 1024
        ),
        name="layer",
    )(
        tokens, w_query, w_key, w_value, w_delta_gate, w_glu_value, w_glu_gate, w_conv_gate,
        w_beta.T, w_decay.T, decay_log, head_gain.reshape(1, 128), conv_taps,
        ln_gain.reshape(1, 128), ln_shift.reshape(1, 128), out_delta, out_conv,
    )


def solution(mesh):
    cut = P(None, "tp")
    placed = (P("sp", "tp"),) + (cut,) * 7 + (P(),) * 4 + (
        cut, P("tp"), P("tp"), P("tp", None), P("tp", None),
    )
    return jax.shard_map(
        local, mesh=mesh, in_specs=placed, out_specs=P(("sp", "tp"), None), check_vma=False
    )
```

```python
import jax
import jax.numpy as jnp
from jax import lax
from jax.experimental import pallas as pl
from jax.experimental.pallas import tpu as pltpu
from jax.sharding import PartitionSpec as P

BF = jnp.bfloat16
F32 = jnp.float32
ROWS = 1024
SHARD = 256
BLK = 128
CHUNK = 256
CHUNKS = ROWS // CHUNK
HALF = CHUNK // 2
COLS = 8 * 128
SEMS = (
    ("w", "wo", "x", "out", "gs", "ms", "xs", "zs1", "zs2", "zs3", "fs", "hs", "ss", "ds", "cs")
    + tuple(f"g{k}{r}" for k in range(3) for r in range(CHUNKS))
    + ("a", "af", "by", "bf", "b0", "b1", "bx", "bm", "zy", "zf", "z0", "zx", "zm")
    + ("xr", "zr1", "zr2", "zr3", "fr", "hr", "sr", "dr", "cr")
)
TAPS = 31
FAR_FIRST = (4, 5, 3, 2, 6, 1, 7)
NORM = 1e-06
VAR = 1e-05
NN = ((1,), (0,))
NT = ((1,), (1,))
TN = ((0,), (0,))


def mm(a, b, dims=NN):
    return lax.dot_general(
        a.astype(BF), b.astype(BF), (dims, ((), ())), preferred_element_type=F32
    )


def iotas(shape):
    return lax.broadcasted_iota(jnp.int32, shape, 0), lax.broadcasted_iota(jnp.int32, shape, 1)


def softplus(v):
    return jnp.maximum(v, 0.0) + jnp.log1p(jnp.exp(-jnp.abs(v)))


def sigmoid(v):
    return jax.nn.sigmoid(v)


def unit_rows(v):
    return v * lax.rsqrt(jnp.sum(v * v, axis=-1, keepdims=True) + NORM)


def block_inverse(lows):
    row, col = iotas((BLK, BLK))
    eye = (row == col).astype(F32)
    parts = [eye - jnp.where((row // 2 == col // 2), low, 0.0) for low in lows]
    m = 2
    while m < BLK:
        pick = (row // (2 * m) == col // (2 * m)) & (row // m != col // m)
        packed = [p.astype(BF) for p in parts]
        inner = [mm(jnp.where(pick, low, 0.0), p) for low, p in zip(lows, packed)]
        parts = [t - mm(p, i) for t, p, i in zip(parts, packed, inner)]
        m *= 2
    return parts


def kernel(
    x, wq, wk, wv, wdg, wgv, wgg, wcg, wb, wd, dlog, hgain, taps, lng, lns, od, oc,
    out,
    xg, w, wo, qs, ks, vs, dgs, cgs, bes, lds, pad, filt, qcs, ocs, mn, mnx, mnz, s4s, s4r,
    halo_s, halo_r, sts, str_, dms, cms, dmr, cmr, stage, half,
    sems, ack,
):
    sp = lax.axis_index("sp")
    t = lax.axis_index("tp")
    y, c = t // 2, t % 2
    z, xx = sp // 4, sp % 4
    zq, zi = z // 4, z % 4
    right = ((y + 1) % 4) * 2 + c
    left = ((y + 3) % 4) * 2 + c
    opp = ((y + 2) % 4) * 2 + c
    mate = y * 2 + (1 - c)

    def at_tp(k):
        return {"sp": sp, "tp": k}

    def at_sp(k):
        return {"sp": k, "tp": t}

    def sem(name):
        return sems.at[SEMS.index(name)]

    def await_bytes(ref, name):
        pltpu.make_async_copy(ref, ref, sem(name)).wait()

    wrefs = (wq, wk, wv, wdg, wgv, wgg, wcg)
    wcopies = [
        pltpu.make_async_copy(ref, w.at[:, k * 128 : (k + 1) * 128], sem("w"))
        for k, ref in enumerate(wrefs)
    ]
    own_rows = pl.ds(pl.multiple_of(t * 128, 128), 128)
    wcopies.append(pltpu.make_async_copy(od, wo.at[0, own_rows, :], sem("wo")))
    wcopies.append(pltpu.make_async_copy(oc, wo.at[1, own_rows, :], sem("wo")))

    def cols_of(k):
        return pl.ds(pl.multiple_of(k * SHARD, SHARD), SHARD)

    xcopy = pltpu.make_async_copy(x, xg.at[:, cols_of(t)], sem("x"))
    xcopy.start()
    for cp in wcopies:
        cp.start()

    mnz[...] = jnp.zeros(mnz.shape, BF)
    s4r[...] = jnp.zeros(s4r.shape, BF)
    halo_r[...] = jnp.zeros(halo_r.shape, BF)
    bar = pltpu.get_barrier_semaphore()

    def signal(semaphore, peer):
        pl.semaphore_signal(
            semaphore, inc=1, device_id=peer, device_id_type=pl.DeviceIdType.MESH
        )

    def signal_if(condition, semaphore, peer):
        @pl.when(condition)
        def _():
            signal(semaphore, peer)

    for d in range(1, 8):
        signal(bar, at_tp((t + d) % 8))
    for d in range(1, 4):
        signal(bar, at_sp(z * 4 + (xx + d) % 4))
    for d in range(1, 4):
        signal_if(zi + d < 4, bar, at_sp((sp + 4 * d) % 32))
    for d in range(1, 5):
        signal_if(z == 3, bar, at_sp((sp + 4 * d) % 32))
    signal_if(z < 7, bar, at_sp((sp + 4) % 32))
    signal_if(z == 0, bar, at_sp((sp + 28) % 32))
    signal_if((xx == 3) & (z < 7), bar, at_sp((sp + 1) % 32))

    def count(*conditions):
        return sum(jnp.where(condition, 1, 0) for condition in conditions)

    pl.semaphore_wait(bar, 10 + zi + count(z >= 4, z > 0, z == 7, (xx == 0) & (z > 0)))
    for d in range(1, 4):
        signal_if(zi - d >= 0, ack, at_sp((sp + 32 - 4 * d) % 32))
    signal_if(z >= 4, ack, at_sp(12 + xx))
    signal_if(z > 0, ack, at_sp((sp + 28) % 32))
    signal_if(z == 7, ack, at_sp((sp + 4) % 32))
    signal_if((xx == 0) & (z > 0), ack, at_sp((sp + 31) % 32))

    def send(src, dst, ssem, rsem, to):
        return pltpu.make_async_remote_copy(
            src_ref=src, dst_ref=dst, send_sem=ssem, recv_sem=rsem,
            device_id=to, device_id_type=pl.DeviceIdType.MESH,
        )

    def gat(kind, r):
        base = r * CHUNK
        whole = pl.ds(pl.multiple_of(base, CHUNK), CHUNK)
        first = pl.ds(pl.multiple_of(base, HALF), HALF)
        second = pl.ds(pl.multiple_of(base + HALF, HALF), HALF)
        rows = (whole, whole, whole, first, second, whole, whole, first, second)[kind]
        shard = (t, t, t, left, right, left, right, opp, opp)[kind]
        to = (right, left, mate, right, left, mate, mate, mate, mate)[kind]
        dst = xg.at[rows, cols_of(shard)]
        return send(dst, dst, sem("gs"), sem(f"g{(0, 0, 2, 1, 1, 2, 2, 2, 2)[kind]}{r}"), at_tp(to))

    def own(r):
        for kind in (0, 1, 2):
            gat(kind, r).start()

    def relay1(r):
        await_bytes(xg.at[0:CHUNK, 0:512], f"g0{r}")
        for kind in (3, 4, 5, 6):
            gat(kind, r).start()

    def relay2(r):
        await_bytes(xg.at[0:CHUNK, 0:256], f"g1{r}")
        gat(7, r).start()
        gat(8, r).start()

    def rows_of(shard, off, n):
        return pl.ds(pl.multiple_of(shard * 128 + off, 8), n)

    near = (left, right, opp)
    xr_id = at_sp(z * 4 + (xx + 1) % 4)
    xl_id = at_sp(z * 4 + (xx + 3) % 4)
    zr_id = at_sp(((z + 1) % 8) * 4 + xx)
    zl_id = at_sp(((z + 7) % 8) * 4 + xx)
    moves = {"m": (wo.at[:, rows_of(t, 0, 128), :], at_tp(mate))}
    a_own = wo.at[0, rows_of(t, 0, 64), :]
    moves["ar"] = (a_own, at_tp(right))
    moves["al"] = (a_own, at_tp(left))
    moves["afr"] = (wo.at[0, rows_of(left, 0, 32), :], at_tp(right))
    moves["afl"] = (wo.at[0, rows_of(right, 32, 32), :], at_tp(left))
    for j in range(3):
        moves["am", j] = (wo.at[0, rows_of(near[j], 0, 64), :], at_tp(mate))

    def spread_moves(name, w_at, base, piece, place, to_right, to_left):
        def part(shard, off, n):
            return wo.at[w_at, rows_of(shard, base + off, n), :]

        half = piece // 2
        mine = piece * place
        before, after = piece * ((place + 3) % 4), piece * ((place + 1) % 4)
        moves[name, "yr"] = (part(t, mine, piece), at_tp(right))
        moves[name, "yl"] = (part(t, mine, piece), at_tp(left))
        moves[name, "yfr"] = (part(left, mine, half), at_tp(right))
        moves[name, "yfl"] = (part(right, mine + half, half), at_tp(left))
        for j in range(3):
            shard = near[j]
            moves[name, "r", j] = (part(shard, mine, piece), to_right)
            moves[name, "l", j] = (part(shard, mine, piece), to_left)
            moves[name, "fr", j] = (part(shard, before, half), to_right)
            moves[name, "fl", j] = (part(shard, after + half, half), to_left)
            across = piece * ((place + 2) % 4)
            for k, off in enumerate((mine, before, after, across)):
                moves[name, f"m{k}", j] = (part(shard, off, piece), at_tp(mate))

    spread_moves("b", 1, 0, 32, xx, xr_id, xl_id)
    spread_moves("z", 0, 64, 16, zi, zr_id, zl_id)

    def go(name, *tags):
        for tag in tags:
            for key in [k for k in moves if k[:2] == (name, tag)]:
                move(*key).start()

    def landing(key):
        if key == "m":
            return "bm"
        if isinstance(key, str):
            return "a" if key in ("ar", "al") else "af"
        name, tag = key[:2]
        if name == "am":
            return "zm"
        if tag in ("yr", "yl"):
            return name + "y"
        if tag in ("yfr", "yfl"):
            return name + "f"
        if tag in ("r", "l"):
            return name + ("1" if name == "b" and key[2] > 0 else "0")
        return name + ("x" if tag in ("fr", "fl") else "m")

    def move(*key):
        key = key if len(key) > 1 else key[0]
        ref, to = moves[key]
        return send(ref, ref, sem("ms"), sem(landing(key)), to)

    def got(name, rows):
        await_bytes(wo.at[0, 0:rows, :], name)

    xcopy.wait()
    own(0)
    own(1)

    pick = (lax.broadcasted_iota(jnp.int32, (8, 128), 0) == t).astype(BF)
    lane = lax.broadcasted_iota(jnp.int32, (8, 128), 1)
    w[:, 896:1024] = (
        mm(wb[...], jnp.where(lane < 64, pick, 0), TN)
        + mm(wd[...], jnp.where(lane < 64, 0, pick), TN)
    ).astype(BF)
    rate = jnp.exp(jnp.full((1, 128), dlog[t], F32))
    row, col = iotas((BLK, BLK))
    causal = row >= col
    strict = row > col
    tri = causal.astype(F32)
    mn[:, :128] = (row == col).astype(F32)
    mn[:, 128:] = jnp.zeros((BLK, BLK), F32)

    await_bytes(w.at[:, :896], "w")

    def project(r):
        rows = slice(r * CHUNK, (r + 1) * CHUNK)
        xr_ = xg[rows, :]
        xf = xr_.astype(F32)
        inv = lax.rsqrt(jnp.sum(xf * xf, axis=1, keepdims=True) / 2048.0 + NORM)
        raw = []
        for n in range(0, COLS, 256):
            d = jnp.dot(xr_, w[:, n : n + 256], preferred_element_type=F32) * inv
            raw += [d[:, :128], d[:, 128:]]
        q, k, v, dg, gv, gg, cg = [a.astype(BF).astype(F32) for a in raw[:7]]
        qs[rows, :] = unit_rows(q) * (128.0 ** -0.5)
        ks[rows, :] = unit_rows(k)
        vs[rows, :] = v
        dgs[rows, :] = dg * sigmoid(dg)
        cgs[rows, :] = cg * sigmoid(cg)
        turned = pltpu.roll(raw[7], 64, 1)
        low_lanes = lax.broadcasted_iota(jnp.int32, (CHUNK, 128), 1) < 64
        bes[rows, :] = sigmoid(jnp.where(low_lanes, raw[7], turned))
        lds[rows, :] = -rate * softplus(jnp.where(low_lanes, turned, raw[7]))
        below = slice(r * CHUNK + 32, (r + 1) * CHUNK + 32)
        pad[below, :] = (gv * sigmoid(gg)).astype(BF).astype(F32)

    def delta(first, last, mid=None):
        spans = [slice(b * BLK, (b + 1) * BLK) for b in range(first, last)]
        sums, lows, scores = [], [], []
        for rows in spans:
            total = lax.dot_general(
                tri, lds[rows, :], (NN, ((), ())),
                precision=lax.Precision.HIGHEST, preferred_element_type=F32,
            )
            spread = total - total.T
            damp = jnp.where(causal, jnp.exp(jnp.where(causal, spread, 0.0)), 0.0)
            kb = ks[rows, :].astype(BF)
            both = mm(jnp.concatenate([kb, qs[rows, :].astype(BF)], axis=0), kb, NT)
            lows.append(jnp.where(strict, both[:BLK] * bes[rows, :] * damp, 0.0))
            scores.append(both[BLK:] * damp)
            sums.append(total)
        inverses = block_inverse(lows)
        if mid is not None:
            mid()
        later = []
        for rows, total, score, inv in zip(spans, sums, scores, inverses):
            grow = jnp.exp(total)
            kv, be = ks[rows, :], bes[rows, :]
            rhs = jnp.concatenate([vs[rows, :] * be, kv * be * grow], axis=1)
            solved = mm(inv, rhs).astype(BF)
            mixed = mm(score, solved)
            tail = total[BLK - 1 : BLK, :]
            fresh = mm(kv * jnp.exp(tail - total), solved, TN)
            later.append(
                (
                    jnp.concatenate([qs[rows, :] * grow - mixed[:, 128:], fresh[:, 128:]], axis=0),
                    mixed[:, :128], fresh[:, :128], jnp.exp(tail),
                )
            )
        state = mn[...]
        for rows, (lhs, o_here, n_here, fade) in zip(spans, later):
            moved = mm(lhs, state)
            qcs[rows, :] = moved[:BLK, :128]
            ocs[rows, :] = moved[:BLK, 128:] + o_here
            m_next = state[:, :128] * fade - moved[BLK:, :128]
            n_next = state[:, 128:] * fade - moved[BLK:, 128:] + n_here
            state = jnp.concatenate([m_next, n_next], axis=1)
        mn[...] = state

    def arrive(r):
        await_bytes(xg.at[0:CHUNK, 0:1024], f"g2{r}")

    relay1(0)
    own(2)
    relay1(1)
    own(3)
    relay2(0)
    await_bytes(wo.at[:, 0:128, :], "wo")

    arrive(0)
    project(0)
    relay1(2)
    delta(0, 2, lambda: relay2(1))
    relay1(3)
    arrive(1)
    project(1)

    def middle():
        relay2(2)
        go("b", "yr", "yl")
        go("z", "yr", "yl")

    delta(2, 4, middle)
    relay2(3)
    move("m").start()
    arrive(2)
    project(2)
    arrive(3)
    project(3)
    delta(4, 8)
    own_x = mn[...].astype(BF)
    mnx[xx] = own_x

    def xsend(d):
        return send(mnx.at[xx], mnx.at[xx], sem("xs"), sem("xr"),
                    at_sp(z * 4 + (xx + d) % 4))

    for d in (1, 2, 3):
        xsend(d).start()
    halo_s[...] = pad[ROWS : ROWS + 32, :].astype(BF)
    hcopy = send(halo_s, halo_r, sem("hs"), sem("hr"), at_sp((sp + 1) % 32))

    @pl.when(z < 7)
    def _():
        pl.semaphore_wait(
            ack, 3 - zi + 1 + count(z == 0, xx == 3) + 4 * count(z == 3)
        )

    @pl.when(sp < 31)
    def _():
        hcopy.start()

    for name, rows in (("b", 64), ("z", 32)):
        got(name + "y", rows)
        go(name, "yfr", "yfl")
        for j in (0, 1):
            move(name, "r", j).start()
            move(name, "l", j).start()
            move(name, "m0", j).start()
    move("ar").start()
    move("al").start()

    tapf = taps[...].astype(F32)

    def conv_rows(i):
        acc = jnp.zeros((64, 128), F32)
        for j in range(TAPS):
            acc = acc + pad[pl.ds(i * 64 + 2 + j, 64), :] * tapf[j : j + 1, :]
        filt[pl.ds(pl.multiple_of(i * 64, 64), 64), :] = acc

    @pl.loop(1, ROWS // 64)
    def _(i):
        conv_rows(i)

    @pl.when(sp > 0)
    def _():
        hcopy.wait_recv()

    keep = (sp > 0).astype(F32)
    pad[0:32, :] = halo_r[...].astype(F32) * keep
    conv_rows(0)
    for b in range(ROWS // BLK):
        lanes = slice(b * BLK, (b + 1) * BLK)
        ft = filt[lanes, :].T
        sts[0:1, lanes] = jnp.sum(ft, axis=0, keepdims=True)
        sts[1:2, lanes] = jnp.sum(ft * ft, axis=0, keepdims=True)

    def ssend(d):
        return send(sts, str_.at[t], sem("ss"), sem("sr"), at_tp((t + d) % 8))

    for d in range(1, 8):
        ssend(d).start()
    str_[t] = sts[...]

    def chain(slots, mine):
        total = slots[0].astype(F32)
        m_in = jnp.where(mine > 0, total[:, :128], (row == col).astype(F32))
        n_in = jnp.where(mine > 0, total[:, 128:], 0.0)
        for k in (1, 2, 3):
            piece = slots[k]
            moved = mm(piece[:, :128], total)
            total = jnp.concatenate(
                [moved[:, :128], moved[:, 128:] + piece[:, 128:].astype(F32)], axis=1
            )
            if k < 3:
                m_in = jnp.where(mine > k, total[:, :128], m_in)
                n_in = jnp.where(mine > k, total[:, 128:], n_in)
        return m_in, n_in, total

    await_bytes(mnx.at[0:3], "xr")
    mxp, nxp, xtotal = chain(mnx, xx)
    mnz[zi] = xtotal.astype(BF)

    def zsend(d):
        return send(mnz.at[zi], mnz.at[zi], sem(f"zs{d}"), sem(f"zr{d}"), at_sp((sp + 4 * d) % 32))

    def upward(d, act):
        @pl.when(zi + d < 4)
        def _():
            act(zsend(d))

    for d in (1, 2, 3):
        upward(d, lambda copy: copy.start())

    got("bf", 32)
    got("zf", 16)
    for name in ("b", "z"):
        for tag in ("r", "l", "m0"):
            move(name, tag, 2).start()
    got("b0", 64)
    for tag in ("fr", "fl", "m1", "m2"):
        move("b", tag, 0).start()
    await_bytes(str_.at[0:7], "sr")
    both = str_[0]
    for k in range(1, 8):
        both = both + str_[k]
    center = both[0:1, :] / 1024.0
    variance = jnp.maximum(both[1:2, :] / 1024.0 - center * center, 0.0)
    scale = lax.rsqrt(variance + VAR)
    for b in range(ROWS // BLK):
        lanes = slice(b * BLK, (b + 1) * BLK)
        cen = jnp.broadcast_to(center[:, lanes], (BLK, BLK)).T
        sca = jnp.broadcast_to(scale[:, lanes], (BLK, BLK)).T
        normed = (filt[lanes, :] - cen) * sca * lng[...] + lns[...]
        cms[lanes, :] = (normed * sigmoid(normed) * cgs[lanes, :]).astype(BF)

    def a2a(src, dst, s_sem, r_sem, d):
        to = (t + d) % 8
        rows = pl.ds(pl.multiple_of(to * BLK, BLK), BLK)
        return send(src.at[rows, :], dst.at[t], sem(s_sem), sem(r_sem), at_tp(to))

    for d in FAR_FIRST:
        a2a(cms, cmr, "cs", "cr", d).start()
    cmr[t] = cms[own_rows, :]
    got("a", 128)
    for key in ("afr", "afl"):
        move(key).start()
    move("am", 0).start()
    move("am", 1).start()

    for d in (1, 2, 3):
        @pl.when(zi - d >= 0)
        def _():
            zsend(d).wait_recv()

    mzp, nzp, ztotal = chain(mnz, zi)
    s4s[...] = ztotal[:, 128:].astype(BF)

    def fcopy(d):
        return send(s4s, s4r, sem("fs"), sem("fr"), at_sp((sp + 4 * d) % 32))

    @pl.when(z == 3)
    def _():
        for d in (4, 3, 2, 1):
            fcopy(d).start()

    moved = mm(mxp, jnp.concatenate([mzp, nzp], axis=1))
    mpre, npre = moved[:, :128], moved[:, 128:] + nxp
    got("b1", 128)
    for j in (1, 2):
        for tag in ("fr", "fl", "m1", "m2"):
            move("b", tag, j).start()
    got("z0", 96)
    go("z", "fr", "fl", "m1", "m2")
    @pl.when(z >= 4)
    def _():
        fcopy(1).wait_recv()

    begin = s4r[...].astype(F32) * (zq > 0).astype(F32)
    carried = mm(mpre, begin) + npre

    for i, d in enumerate(FAR_FIRST + (0,)):
        lanes = pl.ds(pl.multiple_of(lax.rem(t + d, 8) * BLK, BLK), BLK)
        o = ocs[lanes, :] + mm(qcs[lanes, :], carried)
        o = o * lax.rsqrt(jnp.mean(o * o, axis=-1, keepdims=True) + NORM) * hgain[...]
        dms[lanes, :] = (o * dgs[lanes, :]).astype(BF)
        if i in (3, 7):
            for e in FAR_FIRST[max(i - 4, 0) : i]:
                a2a(dms, dmr, "ds", "dr", e).start()
    dmr[t] = dms[own_rows, :]

    got("bx", 96)
    go("b", "m3")
    got("zx", 48)
    go("z", "m3")
    got("af", 64)
    move("am", 2).start()
    await_bytes(cmr.at[0:7], "cr")
    got("bm", 640)
    lhs_c = jnp.concatenate([cmr[k] for k in range(8)], axis=1)

    @pl.loop(0, 8)
    def _(n):
        lanes = pl.ds(pl.multiple_of(n * 256, 256), 256)
        half[n] = jnp.dot(lhs_c, wo[1, :, lanes], preferred_element_type=F32)

    got("zm", 384)
    await_bytes(dmr.at[0:7], "dr")

    lhs_d = jnp.concatenate([dmr[k] for k in range(8)], axis=1)

    def ocopy(n):
        lanes = pl.ds(pl.multiple_of(n * 256, 256), 256)
        return pltpu.make_async_copy(stage.at[n], out.at[:, lanes], sem("out"))

    @pl.loop(0, 8)
    def _(n):
        lanes = pl.ds(pl.multiple_of(n * 256, 256), 256)
        acc = jnp.dot(lhs_d, wo[0, :, lanes], preferred_element_type=F32)
        stage[n] = (acc + half[n]).astype(BF)
        ocopy(n).start()

    await_bytes(stage, "out")
    await_bytes(xg.at[0:896, :], "gs")
    await_bytes(wo.at[:, 0:896, :], "ms")
    await_bytes(mnx.at[0:3], "xs")
    for d in (1, 2, 3):
        upward(d, lambda copy: copy.wait_send())

    @pl.when(z == 3)
    def _():
        await_bytes(mnx.at[0:2], "fs")


    @pl.when(sp < 31)
    def _():
        await_bytes(halo_s, "hs")

    await_bytes(str_.at[0:7], "ss")
    await_bytes(dmr.at[0:7], "ds")
    await_bytes(cmr.at[0:7], "cs")


def local(*args):
    (tokens, w_query, w_key, w_value, w_delta_gate, w_glu_value, w_glu_gate, w_conv_gate,
     w_beta, w_decay, decay_log, head_gain, conv_taps, ln_gain, ln_shift, out_delta,
     out_conv) = args
    vm = pl.BlockSpec(memory_space=pltpu.VMEM)
    hb = pl.BlockSpec(memory_space=pl.ANY)
    sm = pl.BlockSpec(memory_space=pltpu.SMEM)
    big = lambda kind: pltpu.VMEM((ROWS, 128), kind)
    dma = pltpu.SemaphoreType.DMA
    return pl.pallas_call(
        kernel,
        out_shape=jax.ShapeDtypeStruct((BLK, 2048), BF),
        in_specs=[hb] * 8 + [vm, vm, sm] + [vm] * 4 + [hb, hb],
        out_specs=hb,
        scratch_shapes=[
            pltpu.VMEM((ROWS, 2048), BF),
            pltpu.VMEM((2048, COLS), BF),
            pltpu.VMEM((2, 1024, 2048), BF),
            big(F32), big(F32), big(F32), big(F32), big(F32), big(F32), big(F32),
            pltpu.VMEM((ROWS + 32, 128), F32),
            big(F32), big(F32), big(F32),
            pltpu.VMEM((BLK, 256), F32),
            pltpu.VMEM((4, BLK, 256), BF),
            pltpu.VMEM((4, BLK, 256), BF),
            pltpu.VMEM((BLK, BLK), BF),
            pltpu.VMEM((BLK, BLK), BF),
            pltpu.VMEM((32, 128), BF),
            pltpu.VMEM((32, 128), BF),
            pltpu.VMEM((2, ROWS), F32),
            pltpu.VMEM((8, 2, ROWS), F32),
            big(BF), big(BF),
            pltpu.VMEM((8, BLK, BLK), BF),
            pltpu.VMEM((8, BLK, BLK), BF),
            pltpu.VMEM((8, BLK, 256), BF),
            pltpu.VMEM((8, BLK, 256), F32),
            dma((len(SEMS),)),
            pltpu.SemaphoreType.REGULAR,
        ],
        compiler_params=pltpu.CompilerParams(
            collective_id=0, has_side_effects=True, vmem_limit_bytes=60 * 1024 * 1024
        ),
        name="layer",
    )(
        tokens, w_query, w_key, w_value, w_delta_gate, w_glu_value, w_glu_gate, w_conv_gate,
        w_beta.T, w_decay.T, decay_log, head_gain.reshape(1, 128), conv_taps,
        ln_gain.reshape(1, 128), ln_shift.reshape(1, 128), out_delta, out_conv,
    )


def solution(mesh):
    cut = P(None, "tp")
    placed = (P("sp", "tp"),) + (cut,) * 7 + (P(),) * 4 + (
        cut, P("tp"), P("tp"), P("tp", None), P("tp", None),
    )
    return jax.shard_map(
        local, mesh=mesh, in_specs=placed, out_specs=P(("sp", "tp"), None), check_vma=False
    )
```

```python
import jax
import jax.numpy as jnp
from jax import lax
from jax.experimental import pallas as pl
from jax.experimental.pallas import tpu as pltpu
from jax.sharding import PartitionSpec as P

BF = jnp.bfloat16
F32 = jnp.float32
ROWS = 1024
SHARD = 256
BLK = 128
CHUNK = 256
CHUNKS = ROWS // CHUNK
HALF = CHUNK // 2
COLS = 8 * 128
SEMS = (
    ("w", "wo", "x", "out", "gs", "ms", "xs", "zs1", "zs2", "zs3", "fs", "hs", "ss", "ds", "cs")
    + tuple(f"g{k}{r}" for k in range(3) for r in range(CHUNKS))
    + ("a", "af", "by", "bf", "b0", "b1", "bx", "bm", "zy", "zf", "z0", "zx", "zm")
    + ("xr", "zr1", "zr2", "zr3", "fr", "hr", "sr", "dr", "cr")
)
TAPS = 31
FAR_FIRST = (4, 5, 3, 2, 6, 1, 7)
NORM = 1e-06
VAR = 1e-05
NN = ((1,), (0,))
NT = ((1,), (1,))
TN = ((0,), (0,))


def mm(a, b, dims=NN):
    return lax.dot_general(
        a.astype(BF), b.astype(BF), (dims, ((), ())), preferred_element_type=F32
    )


def iotas(shape):
    return lax.broadcasted_iota(jnp.int32, shape, 0), lax.broadcasted_iota(jnp.int32, shape, 1)


def softplus(v):
    return jnp.maximum(v, 0.0) + jnp.log1p(jnp.exp(-jnp.abs(v)))


def sigmoid(v):
    return jax.nn.sigmoid(v)


def unit_rows(v):
    return v * lax.rsqrt(jnp.sum(v * v, axis=-1, keepdims=True) + NORM)


def block_inverse(lows):
    row, col = iotas((BLK, BLK))
    eye = (row == col).astype(F32)
    parts = [eye - jnp.where((row // 2 == col // 2), low, 0.0) for low in lows]
    m = 2
    while m < BLK:
        pick = (row // (2 * m) == col // (2 * m)) & (row // m != col // m)
        packed = [p.astype(BF) for p in parts]
        inner = [mm(jnp.where(pick, low, 0.0), p) for low, p in zip(lows, packed)]
        parts = [t - mm(p, i) for t, p, i in zip(parts, packed, inner)]
        m *= 2
    return parts


def kernel(
    x, wq, wk, wv, wdg, wgv, wgg, wcg, wb, wd, dlog, hgain, taps, lng, lns, od, oc,
    out,
    xg, w, wo, qs, ks, vs, dgs, cgs, bes, lds, pad, filt, qcs, ocs, mn, mnx, mnz, s4s, s4r,
    halo_s, halo_r, sts, str_, dms, cms, dmr, cmr, stage, half,
    sems, ack,
):
    sp = lax.axis_index("sp")
    t = lax.axis_index("tp")
    y, c = t // 2, t % 2
    z, xx = sp // 4, sp % 4
    zq, zi = z // 4, z % 4
    right = ((y + 1) % 4) * 2 + c
    left = ((y + 3) % 4) * 2 + c
    opp = ((y + 2) % 4) * 2 + c
    mate = y * 2 + (1 - c)

    def at_tp(k):
        return {"sp": sp, "tp": k}

    def at_sp(k):
        return {"sp": k, "tp": t}

    def sem(name):
        return sems.at[SEMS.index(name)]

    def await_bytes(ref, name):
        pltpu.make_async_copy(ref, ref, sem(name)).wait()

    wrefs = (wq, wk, wv, wdg, wgv, wgg, wcg)
    wcopies = [
        pltpu.make_async_copy(ref, w.at[:, k * 128 : (k + 1) * 128], sem("w"))
        for k, ref in enumerate(wrefs)
    ]
    own_rows = pl.ds(pl.multiple_of(t * 128, 128), 128)
    wcopies.append(pltpu.make_async_copy(od, wo.at[0, own_rows, :], sem("wo")))
    wcopies.append(pltpu.make_async_copy(oc, wo.at[1, own_rows, :], sem("wo")))

    def cols_of(k):
        return pl.ds(pl.multiple_of(k * SHARD, SHARD), SHARD)

    xcopy = pltpu.make_async_copy(x, xg.at[:, cols_of(t)], sem("x"))
    xcopy.start()
    for cp in wcopies:
        cp.start()

    mnz[...] = jnp.zeros(mnz.shape, BF)
    s4r[...] = jnp.zeros(s4r.shape, BF)
    halo_r[...] = jnp.zeros(halo_r.shape, BF)
    bar = pltpu.get_barrier_semaphore()

    def signal(semaphore, peer):
        pl.semaphore_signal(
            semaphore, inc=1, device_id=peer, device_id_type=pl.DeviceIdType.MESH
        )

    def signal_if(condition, semaphore, peer):
        @pl.when(condition)
        def _():
            signal(semaphore, peer)

    for d in range(1, 8):
        signal(bar, at_tp((t + d) % 8))
    for d in range(1, 4):
        signal(bar, at_sp(z * 4 + (xx + d) % 4))
    for d in range(1, 4):
        signal_if(zi + d < 4, bar, at_sp((sp + 4 * d) % 32))
    for d in range(1, 5):
        signal_if(z == 3, bar, at_sp((sp + 4 * d) % 32))
    signal_if(z < 7, bar, at_sp((sp + 4) % 32))
    signal_if(z == 0, bar, at_sp((sp + 28) % 32))
    signal_if((xx == 3) & (z < 7), bar, at_sp((sp + 1) % 32))

    def count(*conditions):
        return sum(jnp.where(condition, 1, 0) for condition in conditions)

    pl.semaphore_wait(bar, 10 + zi + count(z >= 4, z > 0, z == 7, (xx == 0) & (z > 0)))
    for d in range(1, 4):
        signal_if(zi - d >= 0, ack, at_sp((sp + 32 - 4 * d) % 32))
    signal_if(z >= 4, ack, at_sp(12 + xx))
    signal_if(z > 0, ack, at_sp((sp + 28) % 32))
    signal_if(z == 7, ack, at_sp((sp + 4) % 32))
    signal_if((xx == 0) & (z > 0), ack, at_sp((sp + 31) % 32))

    def send(src, dst, ssem, rsem, to):
        return pltpu.make_async_remote_copy(
            src_ref=src, dst_ref=dst, send_sem=ssem, recv_sem=rsem,
            device_id=to, device_id_type=pl.DeviceIdType.MESH,
        )

    def gat(kind, r):
        base = r * CHUNK
        whole = pl.ds(pl.multiple_of(base, CHUNK), CHUNK)
        first = pl.ds(pl.multiple_of(base, HALF), HALF)
        second = pl.ds(pl.multiple_of(base + HALF, HALF), HALF)
        rows = (whole, whole, whole, first, second, whole, whole, first, second)[kind]
        shard = (t, t, t, left, right, left, right, opp, opp)[kind]
        to = (right, left, mate, right, left, mate, mate, mate, mate)[kind]
        dst = xg.at[rows, cols_of(shard)]
        return send(dst, dst, sem("gs"), sem(f"g{(0, 0, 2, 1, 1, 2, 2, 2, 2)[kind]}{r}"), at_tp(to))

    def own(r):
        for kind in (0, 1, 2):
            gat(kind, r).start()

    def relay1(r):
        await_bytes(xg.at[0:CHUNK, 0:512], f"g0{r}")
        for kind in (3, 4, 5, 6):
            gat(kind, r).start()

    def relay2(r):
        await_bytes(xg.at[0:CHUNK, 0:256], f"g1{r}")
        gat(7, r).start()
        gat(8, r).start()

    def rows_of(shard, off, n):
        return pl.ds(pl.multiple_of(shard * 128 + off, 8), n)

    near = (left, right, opp)
    xr_id = at_sp(z * 4 + (xx + 1) % 4)
    xl_id = at_sp(z * 4 + (xx + 3) % 4)
    zr_id = at_sp(((z + 1) % 8) * 4 + xx)
    zl_id = at_sp(((z + 7) % 8) * 4 + xx)
    moves = {"m": (wo.at[:, rows_of(t, 0, 128), :], at_tp(mate))}
    a_own = wo.at[0, rows_of(t, 0, 64), :]
    moves["ar"] = (a_own, at_tp(right))
    moves["al"] = (a_own, at_tp(left))
    moves["afr"] = (wo.at[0, rows_of(left, 0, 32), :], at_tp(right))
    moves["afl"] = (wo.at[0, rows_of(right, 32, 32), :], at_tp(left))
    for j in range(3):
        moves["am", j] = (wo.at[0, rows_of(near[j], 0, 64), :], at_tp(mate))

    def spread_moves(name, w_at, base, piece, place, to_right, to_left):
        def part(shard, off, n):
            return wo.at[w_at, rows_of(shard, base + off, n), :]

        half = piece // 2
        mine = piece * place
        before, after = piece * ((place + 3) % 4), piece * ((place + 1) % 4)
        moves[name, "yr"] = (part(t, mine, piece), at_tp(right))
        moves[name, "yl"] = (part(t, mine, piece), at_tp(left))
        moves[name, "yfr"] = (part(left, mine, half), at_tp(right))
        moves[name, "yfl"] = (part(right, mine + half, half), at_tp(left))
        for j in range(3):
            shard = near[j]
            moves[name, "r", j] = (part(shard, mine, piece), to_right)
            moves[name, "l", j] = (part(shard, mine, piece), to_left)
            moves[name, "fr", j] = (part(shard, before, half), to_right)
            moves[name, "fl", j] = (part(shard, after + half, half), to_left)
            across = piece * ((place + 2) % 4)
            for k, off in enumerate((mine, before, after, across)):
                moves[name, f"m{k}", j] = (part(shard, off, piece), at_tp(mate))

    spread_moves("b", 1, 0, 32, xx, xr_id, xl_id)
    spread_moves("z", 0, 64, 16, zi, zr_id, zl_id)

    def go(name, *tags):
        for tag in tags:
            for key in [k for k in moves if k[:2] == (name, tag)]:
                move(*key).start()

    def landing(key):
        if key == "m":
            return "bm"
        if isinstance(key, str):
            return "a" if key in ("ar", "al") else "af"
        name, tag = key[:2]
        if name == "am":
            return "zm"
        if tag in ("yr", "yl"):
            return name + "y"
        if tag in ("yfr", "yfl"):
            return name + "f"
        if tag in ("r", "l"):
            return name + ("1" if name == "b" and key[2] > 0 else "0")
        return name + ("x" if tag in ("fr", "fl") else "m")

    def move(*key):
        key = key if len(key) > 1 else key[0]
        ref, to = moves[key]
        return send(ref, ref, sem("ms"), sem(landing(key)), to)

    def got(name, rows):
        await_bytes(wo.at[0, 0:rows, :], name)

    xcopy.wait()
    own(0)
    own(1)

    pick = (lax.broadcasted_iota(jnp.int32, (8, 128), 0) == t).astype(BF)
    lane = lax.broadcasted_iota(jnp.int32, (8, 128), 1)
    w[:, 896:1024] = (
        mm(wb[...], jnp.where(lane < 64, pick, 0), TN)
        + mm(wd[...], jnp.where(lane < 64, 0, pick), TN)
    ).astype(BF)
    rate = jnp.exp(jnp.full((1, 128), dlog[t], F32))
    row, col = iotas((BLK, BLK))
    causal = row >= col
    strict = row > col
    tri = causal.astype(F32)
    mn[:, :128] = (row == col).astype(F32)
    mn[:, 128:] = jnp.zeros((BLK, BLK), F32)

    await_bytes(w.at[:, :896], "w")

    def project(r):
        rows = slice(r * CHUNK, (r + 1) * CHUNK)
        xr_ = xg[rows, :]
        xf = xr_.astype(F32)
        inv = lax.rsqrt(jnp.sum(xf * xf, axis=1, keepdims=True) / 2048.0 + NORM)
        raw = []
        for n in range(0, COLS, 256):
            d = jnp.dot(xr_, w[:, n : n + 256], preferred_element_type=F32) * inv
            raw += [d[:, :128], d[:, 128:]]
        q, k, v, dg, gv, gg, cg = [a.astype(BF).astype(F32) for a in raw[:7]]
        qs[rows, :] = unit_rows(q) * (128.0 ** -0.5)
        ks[rows, :] = unit_rows(k)
        vs[rows, :] = v
        dgs[rows, :] = dg * sigmoid(dg)
        cgs[rows, :] = cg * sigmoid(cg)
        turned = pltpu.roll(raw[7], 64, 1)
        low_lanes = lax.broadcasted_iota(jnp.int32, (CHUNK, 128), 1) < 64
        bes[rows, :] = sigmoid(jnp.where(low_lanes, raw[7], turned))
        lds[rows, :] = -rate * softplus(jnp.where(low_lanes, turned, raw[7]))
        below = slice(r * CHUNK + 32, (r + 1) * CHUNK + 32)
        pad[below, :] = (gv * sigmoid(gg)).astype(BF).astype(F32)

    def delta(first, last, mid=None):
        spans = [slice(b * BLK, (b + 1) * BLK) for b in range(first, last)]
        sums, lows, scores = [], [], []
        for rows in spans:
            total = lax.dot_general(
                tri, lds[rows, :], (NN, ((), ())),
                precision=lax.Precision.HIGHEST, preferred_element_type=F32,
            )
            spread = total - total.T
            damp = jnp.where(causal, jnp.exp(jnp.where(causal, spread, 0.0)), 0.0)
            kb = ks[rows, :].astype(BF)
            both = mm(jnp.concatenate([kb, qs[rows, :].astype(BF)], axis=0), kb, NT)
            lows.append(jnp.where(strict, both[:BLK] * bes[rows, :] * damp, 0.0))
            scores.append(both[BLK:] * damp)
            sums.append(total)
        inverses = block_inverse(lows)
        if mid is not None:
            mid()
        later = []
        for rows, total, score, inv in zip(spans, sums, scores, inverses):
            grow = jnp.exp(total)
            kv, be = ks[rows, :], bes[rows, :]
            rhs = jnp.concatenate([vs[rows, :] * be, kv * be * grow], axis=1)
            solved = mm(inv, rhs).astype(BF)
            mixed = mm(score, solved)
            tail = total[BLK - 1 : BLK, :]
            fresh = mm(kv * jnp.exp(tail - total), solved, TN)
            later.append(
                (
                    jnp.concatenate([qs[rows, :] * grow - mixed[:, 128:], fresh[:, 128:]], axis=0),
                    mixed[:, :128], fresh[:, :128], jnp.exp(tail),
                )
            )
        state = mn[...]
        for rows, (lhs, o_here, n_here, fade) in zip(spans, later):
            moved = mm(lhs, state)
            qcs[rows, :] = moved[:BLK, :128]
            ocs[rows, :] = moved[:BLK, 128:] + o_here
            m_next = state[:, :128] * fade - moved[BLK:, :128]
            n_next = state[:, 128:] * fade - moved[BLK:, 128:] + n_here
            state = jnp.concatenate([m_next, n_next], axis=1)
        mn[...] = state

    def arrive(r):
        await_bytes(xg.at[0:CHUNK, 0:1024], f"g2{r}")

    relay1(0)
    own(2)
    relay1(1)
    own(3)
    relay2(0)
    await_bytes(wo.at[:, 0:128, :], "wo")

    arrive(0)
    project(0)
    relay1(2)
    delta(0, 2, lambda: relay2(1))
    relay1(3)
    arrive(1)
    project(1)

    def middle():
        relay2(2)
        go("b", "yr", "yl")
        go("z", "yr", "yl")

    delta(2, 4, middle)
    relay2(3)
    move("m").start()
    arrive(2)
    project(2)
    arrive(3)
    project(3)
    delta(4, 8)
    own_x = mn[...].astype(BF)
    mnx[xx] = own_x

    def xsend(d):
        return send(mnx.at[xx], mnx.at[xx], sem("xs"), sem("xr"),
                    at_sp(z * 4 + (xx + d) % 4))

    for d in (1, 2, 3):
        xsend(d).start()
    halo_s[...] = pad[ROWS : ROWS + 32, :].astype(BF)
    hcopy = send(halo_s, halo_r, sem("hs"), sem("hr"), at_sp((sp + 1) % 32))

    @pl.when(z < 7)
    def _():
        pl.semaphore_wait(
            ack, 3 - zi + 1 + count(z == 0, xx == 3) + 4 * count(z == 3)
        )

    @pl.when(sp < 31)
    def _():
        hcopy.start()

    for name, rows in (("b", 64), ("z", 32)):
        got(name + "y", rows)
        go(name, "yfr", "yfl")
        for j in (0, 1):
            move(name, "r", j).start()
            move(name, "l", j).start()
            move(name, "m0", j).start()

    tapf = taps[...].astype(F32)

    def conv_rows(i):
        acc = jnp.zeros((64, 128), F32)
        for j in range(TAPS):
            acc = acc + pad[pl.ds(i * 64 + 2 + j, 64), :] * tapf[j : j + 1, :]
        filt[pl.ds(pl.multiple_of(i * 64, 64), 64), :] = acc

    @pl.loop(1, ROWS // 64)
    def _(i):
        conv_rows(i)

    move("ar").start()
    move("al").start()
    @pl.when(sp > 0)
    def _():
        hcopy.wait_recv()

    keep = (sp > 0).astype(F32)
    pad[0:32, :] = halo_r[...].astype(F32) * keep
    conv_rows(0)
    for b in range(ROWS // BLK):
        lanes = slice(b * BLK, (b + 1) * BLK)
        ft = filt[lanes, :].T
        sts[0:1, lanes] = jnp.sum(ft, axis=0, keepdims=True)
        sts[1:2, lanes] = jnp.sum(ft * ft, axis=0, keepdims=True)

    def ssend(d):
        return send(sts, str_.at[t], sem("ss"), sem("sr"), at_tp((t + d) % 8))

    for d in range(1, 8):
        ssend(d).start()
    str_[t] = sts[...]

    def chain(slots, mine):
        total = slots[0].astype(F32)
        m_in = jnp.where(mine > 0, total[:, :128], (row == col).astype(F32))
        n_in = jnp.where(mine > 0, total[:, 128:], 0.0)
        for k in (1, 2, 3):
            piece = slots[k]
            moved = mm(piece[:, :128], total)
            total = jnp.concatenate(
                [moved[:, :128], moved[:, 128:] + piece[:, 128:].astype(F32)], axis=1
            )
            if k < 3:
                m_in = jnp.where(mine > k, total[:, :128], m_in)
                n_in = jnp.where(mine > k, total[:, 128:], n_in)
        return m_in, n_in, total

    got("zf", 16)
    for tag in ("r", "l", "m0"):
        move("z", tag, 2).start()
    await_bytes(mnx.at[0:3], "xr")
    mxp, nxp, xtotal = chain(mnx, xx)
    mnz[zi] = xtotal.astype(BF)

    def zsend(d):
        return send(mnz.at[zi], mnz.at[zi], sem(f"zs{d}"), sem(f"zr{d}"), at_sp((sp + 4 * d) % 32))

    def upward(d, act):
        @pl.when(zi + d < 4)
        def _():
            act(zsend(d))

    for d in (1, 2, 3):
        upward(d, lambda copy: copy.start())

    got("bf", 32)
    for tag in ("r", "l", "m0"):
        move("b", tag, 2).start()
    got("b0", 64)
    for tag in ("fr", "fl", "m1", "m2"):
        move("b", tag, 0).start()
    await_bytes(str_.at[0:7], "sr")
    both = str_[0]
    for k in range(1, 8):
        both = both + str_[k]
    center = both[0:1, :] / 1024.0
    variance = jnp.maximum(both[1:2, :] / 1024.0 - center * center, 0.0)
    scale = lax.rsqrt(variance + VAR)
    for b in range(ROWS // BLK):
        lanes = slice(b * BLK, (b + 1) * BLK)
        cen = jnp.broadcast_to(center[:, lanes], (BLK, BLK)).T
        sca = jnp.broadcast_to(scale[:, lanes], (BLK, BLK)).T
        normed = (filt[lanes, :] - cen) * sca * lng[...] + lns[...]
        cms[lanes, :] = (normed * sigmoid(normed) * cgs[lanes, :]).astype(BF)

    def a2a(src, dst, s_sem, r_sem, d):
        to = (t + d) % 8
        rows = pl.ds(pl.multiple_of(to * BLK, BLK), BLK)
        return send(src.at[rows, :], dst.at[t], sem(s_sem), sem(r_sem), at_tp(to))

    for d in FAR_FIRST:
        a2a(cms, cmr, "cs", "cr", d).start()
    cmr[t] = cms[own_rows, :]
    got("a", 128)
    for key in ("afr", "afl"):
        move(key).start()
    move("am", 0).start()
    move("am", 1).start()

    for d in (1, 2, 3):
        @pl.when(zi - d >= 0)
        def _():
            zsend(d).wait_recv()

    mzp, nzp, ztotal = chain(mnz, zi)
    s4s[...] = ztotal[:, 128:].astype(BF)

    def fcopy(d):
        return send(s4s, s4r, sem("fs"), sem("fr"), at_sp((sp + 4 * d) % 32))

    @pl.when(z == 3)
    def _():
        for d in (4, 3, 2, 1):
            fcopy(d).start()

    moved = mm(mxp, jnp.concatenate([mzp, nzp], axis=1))
    mpre, npre = moved[:, :128], moved[:, 128:] + nxp
    got("b1", 128)
    for j in (1, 2):
        for tag in ("fr", "fl", "m1", "m2"):
            move("b", tag, j).start()
    got("z0", 96)
    go("z", "fr", "fl", "m1", "m2")
    @pl.when(z >= 4)
    def _():
        fcopy(1).wait_recv()

    begin = s4r[...].astype(F32) * (zq > 0).astype(F32)
    carried = mm(mpre, begin) + npre

    for i, d in enumerate(FAR_FIRST + (0,)):
        lanes = pl.ds(pl.multiple_of(lax.rem(t + d, 8) * BLK, BLK), BLK)
        o = ocs[lanes, :] + mm(qcs[lanes, :], carried)
        o = o * lax.rsqrt(jnp.mean(o * o, axis=-1, keepdims=True) + NORM) * hgain[...]
        dms[lanes, :] = (o * dgs[lanes, :]).astype(BF)
        if i in (3, 7):
            for e in FAR_FIRST[max(i - 4, 0) : i]:
                a2a(dms, dmr, "ds", "dr", e).start()
    dmr[t] = dms[own_rows, :]

    got("bx", 96)
    go("b", "m3")
    await_bytes(cmr.at[0:7], "cr")
    got("bm", 640)
    lhs_c = jnp.concatenate([cmr[k] for k in range(8)], axis=1)

    def conv_part(n):
        lanes = pl.ds(pl.multiple_of(n * 256, 256), 256)
        half[n] = jnp.dot(lhs_c, wo[1, :, lanes], preferred_element_type=F32)

    @pl.loop(0, 4)
    def _(n):
        conv_part(n)

    got("af", 64)
    move("am", 2).start()
    got("zx", 48)
    go("z", "m3")
    @pl.loop(4, 8)
    def _(n):
        conv_part(n)

    got("zm", 384)
    await_bytes(dmr.at[0:7], "dr")

    lhs_d = jnp.concatenate([dmr[k] for k in range(8)], axis=1)

    def ocopy(n):
        lanes = pl.ds(pl.multiple_of(n * 256, 256), 256)
        return pltpu.make_async_copy(stage.at[n], out.at[:, lanes], sem("out"))

    @pl.loop(0, 8)
    def _(n):
        lanes = pl.ds(pl.multiple_of(n * 256, 256), 256)
        acc = jnp.dot(lhs_d, wo[0, :, lanes], preferred_element_type=F32)
        stage[n] = (acc + half[n]).astype(BF)
        ocopy(n).start()

    await_bytes(stage, "out")
    await_bytes(xg.at[0:896, :], "gs")
    await_bytes(wo.at[:, 0:896, :], "ms")
    await_bytes(mnx.at[0:3], "xs")
    for d in (1, 2, 3):
        upward(d, lambda copy: copy.wait_send())

    @pl.when(z == 3)
    def _():
        await_bytes(mnx.at[0:2], "fs")


    @pl.when(sp < 31)
    def _():
        await_bytes(halo_s, "hs")

    await_bytes(str_.at[0:7], "ss")
    await_bytes(dmr.at[0:7], "ds")
    await_bytes(cmr.at[0:7], "cs")


def local(*args):
    (tokens, w_query, w_key, w_value, w_delta_gate, w_glu_value, w_glu_gate, w_conv_gate,
     w_beta, w_decay, decay_log, head_gain, conv_taps, ln_gain, ln_shift, out_delta,
     out_conv) = args
    vm = pl.BlockSpec(memory_space=pltpu.VMEM)
    hb = pl.BlockSpec(memory_space=pl.ANY)
    sm = pl.BlockSpec(memory_space=pltpu.SMEM)
    big = lambda kind: pltpu.VMEM((ROWS, 128), kind)
    dma = pltpu.SemaphoreType.DMA
    return pl.pallas_call(
        kernel,
        out_shape=jax.ShapeDtypeStruct((BLK, 2048), BF),
        in_specs=[hb] * 8 + [vm, vm, sm] + [vm] * 4 + [hb, hb],
        out_specs=hb,
        scratch_shapes=[
            pltpu.VMEM((ROWS, 2048), BF),
            pltpu.VMEM((2048, COLS), BF),
            pltpu.VMEM((2, 1024, 2048), BF),
            big(F32), big(F32), big(F32), big(F32), big(F32), big(F32), big(F32),
            pltpu.VMEM((ROWS + 32, 128), F32),
            big(F32), big(F32), big(F32),
            pltpu.VMEM((BLK, 256), F32),
            pltpu.VMEM((4, BLK, 256), BF),
            pltpu.VMEM((4, BLK, 256), BF),
            pltpu.VMEM((BLK, BLK), BF),
            pltpu.VMEM((BLK, BLK), BF),
            pltpu.VMEM((32, 128), BF),
            pltpu.VMEM((32, 128), BF),
            pltpu.VMEM((2, ROWS), F32),
            pltpu.VMEM((8, 2, ROWS), F32),
            big(BF), big(BF),
            pltpu.VMEM((8, BLK, BLK), BF),
            pltpu.VMEM((8, BLK, BLK), BF),
            pltpu.VMEM((8, BLK, 256), BF),
            pltpu.VMEM((8, BLK, 256), F32),
            dma((len(SEMS),)),
            pltpu.SemaphoreType.REGULAR,
        ],
        compiler_params=pltpu.CompilerParams(
            collective_id=0, has_side_effects=True, vmem_limit_bytes=60 * 1024 * 1024
        ),
        name="layer",
    )(
        tokens, w_query, w_key, w_value, w_delta_gate, w_glu_value, w_glu_gate, w_conv_gate,
        w_beta.T, w_decay.T, decay_log, head_gain.reshape(1, 128), conv_taps,
        ln_gain.reshape(1, 128), ln_shift.reshape(1, 128), out_delta, out_conv,
    )


def solution(mesh):
    cut = P(None, "tp")
    placed = (P("sp", "tp"),) + (cut,) * 7 + (P(),) * 4 + (
        cut, P("tp"), P("tp"), P("tp", None), P("tp", None),
    )
    return jax.shard_map(
        local, mesh=mesh, in_specs=placed, out_specs=P(("sp", "tp"), None), check_vma=False
    )
```

```python
import jax
import jax.numpy as jnp
from jax import lax
from jax.experimental import pallas as pl
from jax.experimental.pallas import tpu as pltpu
from jax.sharding import PartitionSpec as P

BF = jnp.bfloat16
F32 = jnp.float32
ROWS = 1024
SHARD = 256
BLK = 128
CHUNK = 256
CHUNKS = ROWS // CHUNK
HALF = CHUNK // 2
COLS = 8 * 128
SEMS = (
    ("w", "wo", "x", "out", "gs", "ms", "xs", "zs1", "zs2", "zs3", "fs", "hs", "ss", "ds", "cs")
    + tuple(f"g{k}{r}" for k in range(3) for r in range(CHUNKS))
    + ("a", "af", "by", "bf", "b0", "b1", "bx", "bm", "zy", "zf", "z0", "zx", "zm")
    + ("xr", "zr1", "zr2", "zr3", "fr", "hr", "sr", "dr", "cr")
)
TAPS = 31
FAR_FIRST = (4, 5, 3, 2, 6, 1, 7)
NORM = 1e-06
VAR = 1e-05
NN = ((1,), (0,))
NT = ((1,), (1,))
TN = ((0,), (0,))


def mm(a, b, dims=NN):
    return lax.dot_general(
        a.astype(BF), b.astype(BF), (dims, ((), ())), preferred_element_type=F32
    )


def iotas(shape):
    return lax.broadcasted_iota(jnp.int32, shape, 0), lax.broadcasted_iota(jnp.int32, shape, 1)


def softplus(v):
    return jnp.maximum(v, 0.0) + jnp.log1p(jnp.exp(-jnp.abs(v)))


def sigmoid(v):
    return jax.nn.sigmoid(v)


def unit_rows(v):
    return v * lax.rsqrt(jnp.sum(v * v, axis=-1, keepdims=True) + NORM)


def block_inverse(lows):
    row, col = iotas((BLK, BLK))
    eye = (row == col).astype(F32)
    parts = [eye - jnp.where((row // 2 == col // 2), low, 0.0) for low in lows]
    m = 2
    while m < BLK:
        pick = (row // (2 * m) == col // (2 * m)) & (row // m != col // m)
        packed = [p.astype(BF) for p in parts]
        inner = [mm(jnp.where(pick, low, 0.0), p) for low, p in zip(lows, packed)]
        parts = [t - mm(p, i) for t, p, i in zip(parts, packed, inner)]
        m *= 2
    return parts


def kernel(
    x, wq, wk, wv, wdg, wgv, wgg, wcg, wb, wd, dlog, hgain, taps, lng, lns, od, oc,
    out,
    xg, w, wo, qs, ks, vs, dgs, cgs, bes, lds, pad, filt, qcs, ocs, mn, mnx, mnz, s4s, s4r,
    halo_s, halo_r, sts, str_, dms, cms, dmr, cmr, stage, half,
    sems, ack,
):
    sp = lax.axis_index("sp")
    t = lax.axis_index("tp")
    y, c = t // 2, t % 2
    z, xx = sp // 4, sp % 4
    zq, zi = z // 4, z % 4
    right = ((y + 1) % 4) * 2 + c
    left = ((y + 3) % 4) * 2 + c
    opp = ((y + 2) % 4) * 2 + c
    mate = y * 2 + (1 - c)

    def at_tp(k):
        return {"sp": sp, "tp": k}

    def at_sp(k):
        return {"sp": k, "tp": t}

    def sem(name):
        return sems.at[SEMS.index(name)]

    def await_bytes(ref, name):
        pltpu.make_async_copy(ref, ref, sem(name)).wait()

    wrefs = (wq, wk, wv, wdg, wgv, wgg, wcg)
    wcopies = [
        pltpu.make_async_copy(ref, w.at[:, k * 128 : (k + 1) * 128], sem("w"))
        for k, ref in enumerate(wrefs)
    ]
    own_rows = pl.ds(pl.multiple_of(t * 128, 128), 128)
    wcopies.append(pltpu.make_async_copy(od, wo.at[0, own_rows, :], sem("wo")))
    wcopies.append(pltpu.make_async_copy(oc, wo.at[1, own_rows, :], sem("wo")))

    def cols_of(k):
        return pl.ds(pl.multiple_of(k * SHARD, SHARD), SHARD)

    xcopy = pltpu.make_async_copy(x, xg.at[:, cols_of(t)], sem("x"))
    xcopy.start()
    for cp in wcopies:
        cp.start()

    mnz[...] = jnp.zeros(mnz.shape, BF)
    s4r[...] = jnp.zeros(s4r.shape, BF)
    halo_r[...] = jnp.zeros(halo_r.shape, BF)
    bar = pltpu.get_barrier_semaphore()

    def signal(semaphore, peer):
        pl.semaphore_signal(
            semaphore, inc=1, device_id=peer, device_id_type=pl.DeviceIdType.MESH
        )

    def signal_if(condition, semaphore, peer):
        @pl.when(condition)
        def _():
            signal(semaphore, peer)

    for d in range(1, 8):
        signal(bar, at_tp((t + d) % 8))
    for d in range(1, 4):
        signal(bar, at_sp(z * 4 + (xx + d) % 4))
    for d in range(1, 4):
        signal_if(zi + d < 4, bar, at_sp((sp + 4 * d) % 32))
    for d in range(1, 5):
        signal_if(z == 3, bar, at_sp((sp + 4 * d) % 32))
    signal_if(z < 7, bar, at_sp((sp + 4) % 32))
    signal_if(z == 0, bar, at_sp((sp + 28) % 32))
    signal_if((xx == 3) & (z < 7), bar, at_sp((sp + 1) % 32))

    def count(*conditions):
        return sum(jnp.where(condition, 1, 0) for condition in conditions)

    pl.semaphore_wait(bar, 10 + zi + count(z >= 4, z > 0, z == 7, (xx == 0) & (z > 0)))
    for d in range(1, 4):
        signal_if(zi - d >= 0, ack, at_sp((sp + 32 - 4 * d) % 32))
    signal_if(z >= 4, ack, at_sp(12 + xx))
    signal_if(z > 0, ack, at_sp((sp + 28) % 32))
    signal_if(z == 7, ack, at_sp((sp + 4) % 32))
    signal_if((xx == 0) & (z > 0), ack, at_sp((sp + 31) % 32))

    def send(src, dst, ssem, rsem, to):
        return pltpu.make_async_remote_copy(
            src_ref=src, dst_ref=dst, send_sem=ssem, recv_sem=rsem,
            device_id=to, device_id_type=pl.DeviceIdType.MESH,
        )

    def gat(kind, r):
        base = r * CHUNK
        whole = pl.ds(pl.multiple_of(base, CHUNK), CHUNK)
        first = pl.ds(pl.multiple_of(base, HALF), HALF)
        second = pl.ds(pl.multiple_of(base + HALF, HALF), HALF)
        rows = (whole, whole, whole, first, second, whole, whole, first, second)[kind]
        shard = (t, t, t, left, right, left, right, opp, opp)[kind]
        to = (right, left, mate, right, left, mate, mate, mate, mate)[kind]
        dst = xg.at[rows, cols_of(shard)]
        return send(dst, dst, sem("gs"), sem(f"g{(0, 0, 2, 1, 1, 2, 2, 2, 2)[kind]}{r}"), at_tp(to))

    def own(r):
        for kind in (0, 1, 2):
            gat(kind, r).start()

    def relay1(r):
        await_bytes(xg.at[0:CHUNK, 0:512], f"g0{r}")
        for kind in (3, 4, 5, 6):
            gat(kind, r).start()

    def relay2(r):
        await_bytes(xg.at[0:CHUNK, 0:256], f"g1{r}")
        gat(7, r).start()
        gat(8, r).start()

    def rows_of(shard, off, n):
        return pl.ds(pl.multiple_of(shard * 128 + off, 8), n)

    near = (left, right, opp)
    xr_id = at_sp(z * 4 + (xx + 1) % 4)
    xl_id = at_sp(z * 4 + (xx + 3) % 4)
    zr_id = at_sp(((z + 1) % 8) * 4 + xx)
    zl_id = at_sp(((z + 7) % 8) * 4 + xx)
    moves = {"m": (wo.at[:, rows_of(t, 0, 128), :], at_tp(mate))}
    a_own = wo.at[0, rows_of(t, 0, 64), :]
    moves["ar"] = (a_own, at_tp(right))
    moves["al"] = (a_own, at_tp(left))
    moves["afr"] = (wo.at[0, rows_of(left, 0, 32), :], at_tp(right))
    moves["afl"] = (wo.at[0, rows_of(right, 32, 32), :], at_tp(left))
    for j in range(3):
        moves["am", j] = (wo.at[0, rows_of(near[j], 0, 64), :], at_tp(mate))

    def spread_moves(name, w_at, base, piece, place, to_right, to_left):
        def part(shard, off, n):
            return wo.at[w_at, rows_of(shard, base + off, n), :]

        half = piece // 2
        mine = piece * place
        before, after = piece * ((place + 3) % 4), piece * ((place + 1) % 4)
        moves[name, "yr"] = (part(t, mine, piece), at_tp(right))
        moves[name, "yl"] = (part(t, mine, piece), at_tp(left))
        moves[name, "yfr"] = (part(left, mine, half), at_tp(right))
        moves[name, "yfl"] = (part(right, mine + half, half), at_tp(left))
        for j in range(3):
            shard = near[j]
            moves[name, "r", j] = (part(shard, mine, piece), to_right)
            moves[name, "l", j] = (part(shard, mine, piece), to_left)
            moves[name, "fr", j] = (part(shard, before, half), to_right)
            moves[name, "fl", j] = (part(shard, after + half, half), to_left)
            across = piece * ((place + 2) % 4)
            for k, off in enumerate((mine, before, after, across)):
                moves[name, f"m{k}", j] = (part(shard, off, piece), at_tp(mate))

    spread_moves("b", 1, 0, 32, xx, xr_id, xl_id)
    spread_moves("z", 0, 64, 16, zi, zr_id, zl_id)

    def go(name, *tags):
        for tag in tags:
            for key in [k for k in moves if k[:2] == (name, tag)]:
                move(*key).start()

    def landing(key):
        if key == "m":
            return "bm"
        if isinstance(key, str):
            return "a" if key in ("ar", "al") else "af"
        name, tag = key[:2]
        if name == "am":
            return "zm"
        if tag in ("yr", "yl"):
            return name + "y"
        if tag in ("yfr", "yfl"):
            return name + "f"
        if tag in ("r", "l"):
            return name + ("1" if name == "b" and key[2] > 0 else "0")
        return name + ("x" if tag in ("fr", "fl") else "m")

    def move(*key):
        key = key if len(key) > 1 else key[0]
        ref, to = moves[key]
        return send(ref, ref, sem("ms"), sem(landing(key)), to)

    def got(name, rows):
        await_bytes(wo.at[0, 0:rows, :], name)

    xcopy.wait()
    own(0)
    own(1)

    pick = (lax.broadcasted_iota(jnp.int32, (8, 128), 0) == t).astype(BF)
    lane = lax.broadcasted_iota(jnp.int32, (8, 128), 1)
    w[:, 896:1024] = (
        mm(wb[...], jnp.where(lane < 64, pick, 0), TN)
        + mm(wd[...], jnp.where(lane < 64, 0, pick), TN)
    ).astype(BF)
    rate = jnp.exp(jnp.full((1, 128), dlog[t], F32))
    row, col = iotas((BLK, BLK))
    causal = row >= col
    strict = row > col
    tri = causal.astype(F32)
    mn[:, :128] = (row == col).astype(F32)
    mn[:, 128:] = jnp.zeros((BLK, BLK), F32)

    await_bytes(w.at[:, :896], "w")

    def project(r):
        rows = slice(r * CHUNK, (r + 1) * CHUNK)
        xr_ = xg[rows, :]
        xf = xr_.astype(F32)
        inv = lax.rsqrt(jnp.sum(xf * xf, axis=1, keepdims=True) / 2048.0 + NORM)
        raw = []
        for n in range(0, COLS, 256):
            d = jnp.dot(xr_, w[:, n : n + 256], preferred_element_type=F32) * inv
            raw += [d[:, :128], d[:, 128:]]
        q, k, v, dg, gv, gg, cg = [a.astype(BF).astype(F32) for a in raw[:7]]
        qs[rows, :] = unit_rows(q) * (128.0 ** -0.5)
        ks[rows, :] = unit_rows(k)
        vs[rows, :] = v
        dgs[rows, :] = dg * sigmoid(dg)
        cgs[rows, :] = cg * sigmoid(cg)
        turned = pltpu.roll(raw[7], 64, 1)
        low_lanes = lax.broadcasted_iota(jnp.int32, (CHUNK, 128), 1) < 64
        bes[rows, :] = sigmoid(jnp.where(low_lanes, raw[7], turned))
        lds[rows, :] = -rate * softplus(jnp.where(low_lanes, turned, raw[7]))
        below = slice(r * CHUNK + 32, (r + 1) * CHUNK + 32)
        pad[below, :] = (gv * sigmoid(gg)).astype(BF).astype(F32)

    def delta(first, last, mid=None):
        spans = [slice(b * BLK, (b + 1) * BLK) for b in range(first, last)]
        sums, lows, scores = [], [], []
        for rows in spans:
            total = lax.dot_general(
                tri, lds[rows, :], (NN, ((), ())),
                precision=lax.Precision.HIGHEST, preferred_element_type=F32,
            )
            spread = total - total.T
            damp = jnp.where(causal, jnp.exp(jnp.where(causal, spread, 0.0)), 0.0)
            kb = ks[rows, :].astype(BF)
            both = mm(jnp.concatenate([kb, qs[rows, :].astype(BF)], axis=0), kb, NT)
            lows.append(jnp.where(strict, both[:BLK] * bes[rows, :] * damp, 0.0))
            scores.append(both[BLK:] * damp)
            sums.append(total)
        inverses = block_inverse(lows)
        if mid is not None:
            mid()
        later = []
        for rows, total, score, inv in zip(spans, sums, scores, inverses):
            grow = jnp.exp(total)
            kv, be = ks[rows, :], bes[rows, :]
            rhs = jnp.concatenate([vs[rows, :] * be, kv * be * grow], axis=1)
            solved = mm(inv, rhs).astype(BF)
            mixed = mm(score, solved)
            tail = total[BLK - 1 : BLK, :]
            fresh = mm(kv * jnp.exp(tail - total), solved, TN)
            later.append(
                (
                    jnp.concatenate([qs[rows, :] * grow - mixed[:, 128:], fresh[:, 128:]], axis=0),
                    mixed[:, :128], fresh[:, :128], jnp.exp(tail),
                )
            )
        state = mn[...]
        for rows, (lhs, o_here, n_here, fade) in zip(spans, later):
            moved = mm(lhs, state)
            qcs[rows, :] = moved[:BLK, :128]
            ocs[rows, :] = moved[:BLK, 128:] + o_here
            m_next = state[:, :128] * fade - moved[BLK:, :128]
            n_next = state[:, 128:] * fade - moved[BLK:, 128:] + n_here
            state = jnp.concatenate([m_next, n_next], axis=1)
        mn[...] = state

    def arrive(r):
        await_bytes(xg.at[0:CHUNK, 0:1024], f"g2{r}")

    relay1(0)
    own(2)
    relay1(1)
    own(3)
    relay2(0)
    await_bytes(wo.at[:, 0:128, :], "wo")

    arrive(0)
    project(0)
    relay1(2)
    delta(0, 2, lambda: relay2(1))
    relay1(3)
    arrive(1)
    project(1)

    def middle():
        relay2(2)
        go("b", "yr", "yl")
        go("z", "yr", "yl")

    delta(2, 4, middle)
    relay2(3)
    move("m").start()
    arrive(2)
    project(2)
    arrive(3)
    project(3)
    delta(4, 8)
    own_x = mn[...].astype(BF)
    mnx[xx] = own_x

    def xsend(d):
        return send(mnx.at[xx], mnx.at[xx], sem("xs"), sem("xr"),
                    at_sp(z * 4 + (xx + d) % 4))

    for d in (1, 2, 3):
        xsend(d).start()
    halo_s[...] = pad[ROWS : ROWS + 32, :].astype(BF)
    hcopy = send(halo_s, halo_r, sem("hs"), sem("hr"), at_sp((sp + 1) % 32))

    @pl.when(z < 7)
    def _():
        pl.semaphore_wait(
            ack, 3 - zi + 1 + count(z == 0, xx == 3) + 4 * count(z == 3)
        )

    @pl.when(sp < 31)
    def _():
        hcopy.start()

    for name, rows in (("b", 64), ("z", 32)):
        got(name + "y", rows)
        go(name, "yfr", "yfl")
        for j in (0, 1):
            move(name, "r", j).start()
            move(name, "l", j).start()
            move(name, "m0", j).start()

    tapf = taps[...].astype(F32)

    def conv_rows(i):
        acc = jnp.zeros((64, 128), F32)
        for j in range(TAPS):
            acc = acc + pad[pl.ds(i * 64 + 2 + j, 64), :] * tapf[j : j + 1, :]
        filt[pl.ds(pl.multiple_of(i * 64, 64), 64), :] = acc

    @pl.loop(1, ROWS // 64)
    def _(i):
        conv_rows(i)

    @pl.when(sp > 0)
    def _():
        hcopy.wait_recv()

    keep = (sp > 0).astype(F32)
    pad[0:32, :] = halo_r[...].astype(F32) * keep
    conv_rows(0)
    for b in range(ROWS // BLK):
        lanes = slice(b * BLK, (b + 1) * BLK)
        ft = filt[lanes, :].T
        sts[0:1, lanes] = jnp.sum(ft, axis=0, keepdims=True)
        sts[1:2, lanes] = jnp.sum(ft * ft, axis=0, keepdims=True)

    def ssend(d):
        return send(sts, str_.at[t], sem("ss"), sem("sr"), at_tp((t + d) % 8))

    for d in range(1, 8):
        ssend(d).start()
    str_[t] = sts[...]

    def chain(slots, mine):
        total = slots[0].astype(F32)
        m_in = jnp.where(mine > 0, total[:, :128], (row == col).astype(F32))
        n_in = jnp.where(mine > 0, total[:, 128:], 0.0)
        for k in (1, 2, 3):
            piece = slots[k]
            moved = mm(piece[:, :128], total)
            total = jnp.concatenate(
                [moved[:, :128], moved[:, 128:] + piece[:, 128:].astype(F32)], axis=1
            )
            if k < 3:
                m_in = jnp.where(mine > k, total[:, :128], m_in)
                n_in = jnp.where(mine > k, total[:, 128:], n_in)
        return m_in, n_in, total

    got("zf", 16)
    for tag in ("r", "l", "m0"):
        move("z", tag, 2).start()
    await_bytes(mnx.at[0:3], "xr")
    mxp, nxp, xtotal = chain(mnx, xx)
    mnz[zi] = xtotal.astype(BF)

    def zsend(d):
        return send(mnz.at[zi], mnz.at[zi], sem(f"zs{d}"), sem(f"zr{d}"), at_sp((sp + 4 * d) % 32))

    def upward(d, act):
        @pl.when(zi + d < 4)
        def _():
            act(zsend(d))

    for d in (1, 2, 3):
        upward(d, lambda copy: copy.start())

    got("bf", 32)
    for tag in ("r", "l", "m0"):
        move("b", tag, 2).start()
    move("ar").start()
    move("al").start()
    got("b0", 64)
    for tag in ("fr", "fl", "m1", "m2"):
        move("b", tag, 0).start()
    await_bytes(str_.at[0:7], "sr")
    both = str_[0]
    for k in range(1, 8):
        both = both + str_[k]
    center = both[0:1, :] / 1024.0
    variance = jnp.maximum(both[1:2, :] / 1024.0 - center * center, 0.0)
    scale = lax.rsqrt(variance + VAR)
    for b in range(ROWS // BLK):
        lanes = slice(b * BLK, (b + 1) * BLK)
        cen = jnp.broadcast_to(center[:, lanes], (BLK, BLK)).T
        sca = jnp.broadcast_to(scale[:, lanes], (BLK, BLK)).T
        normed = (filt[lanes, :] - cen) * sca * lng[...] + lns[...]
        cms[lanes, :] = (normed * sigmoid(normed) * cgs[lanes, :]).astype(BF)

    def a2a(src, dst, s_sem, r_sem, d):
        to = (t + d) % 8
        rows = pl.ds(pl.multiple_of(to * BLK, BLK), BLK)
        return send(src.at[rows, :], dst.at[t], sem(s_sem), sem(r_sem), at_tp(to))

    for d in FAR_FIRST:
        a2a(cms, cmr, "cs", "cr", d).start()
    cmr[t] = cms[own_rows, :]

    for d in (1, 2, 3):
        @pl.when(zi - d >= 0)
        def _():
            zsend(d).wait_recv()

    mzp, nzp, ztotal = chain(mnz, zi)
    s4s[...] = ztotal[:, 128:].astype(BF)

    def fcopy(d):
        return send(s4s, s4r, sem("fs"), sem("fr"), at_sp((sp + 4 * d) % 32))

    @pl.when(z == 3)
    def _():
        for d in (4, 3, 2, 1):
            fcopy(d).start()

    moved = mm(mxp, jnp.concatenate([mzp, nzp], axis=1))
    mpre, npre = moved[:, :128], moved[:, 128:] + nxp
    got("b1", 128)
    for j in (1, 2):
        for tag in ("fr", "fl", "m1", "m2"):
            move("b", tag, j).start()
    got("z0", 96)
    go("z", "fr", "fl", "m1", "m2")
    got("a", 128)
    for key in ("afr", "afl"):
        move(key).start()
    move("am", 0).start()
    move("am", 1).start()
    @pl.when(z >= 4)
    def _():
        fcopy(1).wait_recv()

    begin = s4r[...].astype(F32) * (zq > 0).astype(F32)
    carried = mm(mpre, begin) + npre

    for i, d in enumerate(FAR_FIRST + (0,)):
        lanes = pl.ds(pl.multiple_of(lax.rem(t + d, 8) * BLK, BLK), BLK)
        o = ocs[lanes, :] + mm(qcs[lanes, :], carried)
        o = o * lax.rsqrt(jnp.mean(o * o, axis=-1, keepdims=True) + NORM) * hgain[...]
        dms[lanes, :] = (o * dgs[lanes, :]).astype(BF)
        if i in (3, 7):
            for e in FAR_FIRST[max(i - 4, 0) : i]:
                a2a(dms, dmr, "ds", "dr", e).start()
    dmr[t] = dms[own_rows, :]

    got("bx", 96)
    go("b", "m3")
    await_bytes(cmr.at[0:7], "cr")
    got("bm", 640)
    lhs_c = jnp.concatenate([cmr[k] for k in range(8)], axis=1)

    def conv_part(n):
        lanes = pl.ds(pl.multiple_of(n * 256, 256), 256)
        half[n] = jnp.dot(lhs_c, wo[1, :, lanes], preferred_element_type=F32)

    @pl.loop(0, 4)
    def _(n):
        conv_part(n)

    got("af", 64)
    move("am", 2).start()
    got("zx", 48)
    go("z", "m3")
    @pl.loop(4, 8)
    def _(n):
        conv_part(n)

    got("zm", 384)
    await_bytes(dmr.at[0:7], "dr")

    lhs_d = jnp.concatenate([dmr[k] for k in range(8)], axis=1)

    def ocopy(n):
        lanes = pl.ds(pl.multiple_of(n * 256, 256), 256)
        return pltpu.make_async_copy(stage.at[n], out.at[:, lanes], sem("out"))

    @pl.loop(0, 8)
    def _(n):
        lanes = pl.ds(pl.multiple_of(n * 256, 256), 256)
        acc = jnp.dot(lhs_d, wo[0, :, lanes], preferred_element_type=F32)
        stage[n] = (acc + half[n]).astype(BF)
        ocopy(n).start()

    await_bytes(stage, "out")
    await_bytes(xg.at[0:896, :], "gs")
    await_bytes(wo.at[:, 0:896, :], "ms")
    await_bytes(mnx.at[0:3], "xs")
    for d in (1, 2, 3):
        upward(d, lambda copy: copy.wait_send())

    @pl.when(z == 3)
    def _():
        await_bytes(mnx.at[0:2], "fs")


    @pl.when(sp < 31)
    def _():
        await_bytes(halo_s, "hs")

    await_bytes(str_.at[0:7], "ss")
    await_bytes(dmr.at[0:7], "ds")
    await_bytes(cmr.at[0:7], "cs")


def local(*args):
    (tokens, w_query, w_key, w_value, w_delta_gate, w_glu_value, w_glu_gate, w_conv_gate,
     w_beta, w_decay, decay_log, head_gain, conv_taps, ln_gain, ln_shift, out_delta,
     out_conv) = args
    vm = pl.BlockSpec(memory_space=pltpu.VMEM)
    hb = pl.BlockSpec(memory_space=pl.ANY)
    sm = pl.BlockSpec(memory_space=pltpu.SMEM)
    big = lambda kind: pltpu.VMEM((ROWS, 128), kind)
    dma = pltpu.SemaphoreType.DMA
    return pl.pallas_call(
        kernel,
        out_shape=jax.ShapeDtypeStruct((BLK, 2048), BF),
        in_specs=[hb] * 8 + [vm, vm, sm] + [vm] * 4 + [hb, hb],
        out_specs=hb,
        scratch_shapes=[
            pltpu.VMEM((ROWS, 2048), BF),
            pltpu.VMEM((2048, COLS), BF),
            pltpu.VMEM((2, 1024, 2048), BF),
            big(F32), big(F32), big(F32), big(F32), big(F32), big(F32), big(F32),
            pltpu.VMEM((ROWS + 32, 128), F32),
            big(F32), big(F32), big(F32),
            pltpu.VMEM((BLK, 256), F32),
            pltpu.VMEM((4, BLK, 256), BF),
            pltpu.VMEM((4, BLK, 256), BF),
            pltpu.VMEM((BLK, BLK), BF),
            pltpu.VMEM((BLK, BLK), BF),
            pltpu.VMEM((32, 128), BF),
            pltpu.VMEM((32, 128), BF),
            pltpu.VMEM((2, ROWS), F32),
            pltpu.VMEM((8, 2, ROWS), F32),
            big(BF), big(BF),
            pltpu.VMEM((8, BLK, BLK), BF),
            pltpu.VMEM((8, BLK, BLK), BF),
            pltpu.VMEM((8, BLK, 256), BF),
            pltpu.VMEM((8, BLK, 256), F32),
            dma((len(SEMS),)),
            pltpu.SemaphoreType.REGULAR,
        ],
        compiler_params=pltpu.CompilerParams(
            collective_id=0, has_side_effects=True, vmem_limit_bytes=60 * 1024 * 1024
        ),
        name="layer",
    )(
        tokens, w_query, w_key, w_value, w_delta_gate, w_glu_value, w_glu_gate, w_conv_gate,
        w_beta.T, w_decay.T, decay_log, head_gain.reshape(1, 128), conv_taps,
        ln_gain.reshape(1, 128), ln_shift.reshape(1, 128), out_delta, out_conv,
    )


def solution(mesh):
    cut = P(None, "tp")
    placed = (P("sp", "tp"),) + (cut,) * 7 + (P(),) * 4 + (
        cut, P("tp"), P("tp"), P("tp", None), P("tp", None),
    )
    return jax.shard_map(
        local, mesh=mesh, in_specs=placed, out_specs=P(("sp", "tp"), None), check_vma=False
    )
```

```python
import jax
import jax.numpy as jnp
from jax import lax
from jax.experimental import pallas as pl
from jax.experimental.pallas import tpu as pltpu
from jax.sharding import PartitionSpec as P

BF = jnp.bfloat16
F32 = jnp.float32
ROWS = 1024
SHARD = 256
BLK = 128
CHUNK = 256
CHUNKS = ROWS // CHUNK
HALF = CHUNK // 2
COLS = 8 * 128
SEMS = (
    ("w", "wo", "x", "out", "gs", "ms", "xs", "zs1", "zs2", "zs3", "fs", "hs", "ss", "ds", "cs")
    + tuple(f"g{k}{r}" for k in range(3) for r in range(CHUNKS))
    + ("a", "af", "by", "bf", "b0", "b1", "bx", "bm", "zy", "zf", "z0", "zx", "zm")
    + ("xr", "zr1", "zr2", "zr3", "fr", "hr", "sr", "dr", "cr")
)
TAPS = 31
FAR_FIRST = (4, 5, 3, 2, 6, 1, 7)
NORM = 1e-06
VAR = 1e-05
NN = ((1,), (0,))
NT = ((1,), (1,))
TN = ((0,), (0,))


def mm(a, b, dims=NN):
    return lax.dot_general(
        a.astype(BF), b.astype(BF), (dims, ((), ())), preferred_element_type=F32
    )


def iotas(shape):
    return lax.broadcasted_iota(jnp.int32, shape, 0), lax.broadcasted_iota(jnp.int32, shape, 1)


def softplus(v):
    return jnp.maximum(v, 0.0) + jnp.log1p(jnp.exp(-jnp.abs(v)))


def sigmoid(v):
    return jax.nn.sigmoid(v)


def unit_rows(v):
    return v * lax.rsqrt(jnp.sum(v * v, axis=-1, keepdims=True) + NORM)


def block_inverse(lows):
    row, col = iotas((BLK, BLK))
    eye = (row == col).astype(F32)
    parts = [eye - jnp.where((row // 2 == col // 2), low, 0.0) for low in lows]
    m = 2
    while m < BLK:
        pick = (row // (2 * m) == col // (2 * m)) & (row // m != col // m)
        packed = [p.astype(BF) for p in parts]
        inner = [mm(jnp.where(pick, low, 0.0), p) for low, p in zip(lows, packed)]
        parts = [t - mm(p, i) for t, p, i in zip(parts, packed, inner)]
        m *= 2
    return parts


def kernel(
    x, wq, wk, wv, wdg, wgv, wgg, wcg, wb, wd, dlog, hgain, taps, lng, lns, od, oc,
    out,
    xg, w, wo, qs, ks, vs, dgs, cgs, bes, lds, pad, filt, qcs, ocs, mn, mnx, mnz, s4s, s4r,
    halo_s, halo_r, sts, str_, dms, cms, dmr, cmr, stage, half,
    sems, ack,
):
    sp = lax.axis_index("sp")
    t = lax.axis_index("tp")
    y, c = t // 2, t % 2
    z, xx = sp // 4, sp % 4
    zq, zi = z // 4, z % 4
    right = ((y + 1) % 4) * 2 + c
    left = ((y + 3) % 4) * 2 + c
    opp = ((y + 2) % 4) * 2 + c
    mate = y * 2 + (1 - c)

    def at_tp(k):
        return {"sp": sp, "tp": k}

    def at_sp(k):
        return {"sp": k, "tp": t}

    def sem(name):
        return sems.at[SEMS.index(name)]

    def await_bytes(ref, name):
        pltpu.make_async_copy(ref, ref, sem(name)).wait()

    wrefs = (wq, wk, wv, wdg, wgv, wgg, wcg)
    wcopies = [
        pltpu.make_async_copy(ref, w.at[:, k * 128 : (k + 1) * 128], sem("w"))
        for k, ref in enumerate(wrefs)
    ]
    own_rows = pl.ds(pl.multiple_of(t * 128, 128), 128)
    wcopies.append(pltpu.make_async_copy(od, wo.at[0, own_rows, :], sem("wo")))
    wcopies.append(pltpu.make_async_copy(oc, wo.at[1, own_rows, :], sem("wo")))

    def cols_of(k):
        return pl.ds(pl.multiple_of(k * SHARD, SHARD), SHARD)

    xcopy = pltpu.make_async_copy(x, xg.at[:, cols_of(t)], sem("x"))
    xcopy.start()
    for cp in wcopies:
        cp.start()

    mnz[...] = jnp.zeros(mnz.shape, BF)
    s4r[...] = jnp.zeros(s4r.shape, BF)
    halo_r[...] = jnp.zeros(halo_r.shape, BF)
    bar = pltpu.get_barrier_semaphore()

    def signal(semaphore, peer):
        pl.semaphore_signal(
            semaphore, inc=1, device_id=peer, device_id_type=pl.DeviceIdType.MESH
        )

    def signal_if(condition, semaphore, peer):
        @pl.when(condition)
        def _():
            signal(semaphore, peer)

    for d in range(1, 8):
        signal(bar, at_tp((t + d) % 8))
    for d in range(1, 4):
        signal(bar, at_sp(z * 4 + (xx + d) % 4))
    for d in range(1, 4):
        signal_if(zi + d < 4, bar, at_sp((sp + 4 * d) % 32))
    for d in range(1, 5):
        signal_if(z == 3, bar, at_sp((sp + 4 * d) % 32))
    signal_if(z < 7, bar, at_sp((sp + 4) % 32))
    signal_if(z == 0, bar, at_sp((sp + 28) % 32))
    signal_if((xx == 3) & (z < 7), bar, at_sp((sp + 1) % 32))

    def count(*conditions):
        return sum(jnp.where(condition, 1, 0) for condition in conditions)

    pl.semaphore_wait(bar, 10 + zi + count(z >= 4, z > 0, z == 7, (xx == 0) & (z > 0)))
    for d in range(1, 4):
        signal_if(zi - d >= 0, ack, at_sp((sp + 32 - 4 * d) % 32))
    signal_if(z >= 4, ack, at_sp(12 + xx))
    signal_if(z > 0, ack, at_sp((sp + 28) % 32))
    signal_if(z == 7, ack, at_sp((sp + 4) % 32))
    signal_if((xx == 0) & (z > 0), ack, at_sp((sp + 31) % 32))

    def send(src, dst, ssem, rsem, to):
        return pltpu.make_async_remote_copy(
            src_ref=src, dst_ref=dst, send_sem=ssem, recv_sem=rsem,
            device_id=to, device_id_type=pl.DeviceIdType.MESH,
        )

    def gat(kind, r):
        base = r * CHUNK
        whole = pl.ds(pl.multiple_of(base, CHUNK), CHUNK)
        first = pl.ds(pl.multiple_of(base, HALF), HALF)
        second = pl.ds(pl.multiple_of(base + HALF, HALF), HALF)
        rows = (whole, whole, whole, first, second, whole, whole, first, second)[kind]
        shard = (t, t, t, left, right, left, right, opp, opp)[kind]
        to = (right, left, mate, right, left, mate, mate, mate, mate)[kind]
        dst = xg.at[rows, cols_of(shard)]
        return send(dst, dst, sem("gs"), sem(f"g{(0, 0, 2, 1, 1, 2, 2, 2, 2)[kind]}{r}"), at_tp(to))

    def own(r):
        for kind in (0, 1, 2):
            gat(kind, r).start()

    def relay1(r):
        await_bytes(xg.at[0:CHUNK, 0:512], f"g0{r}")
        for kind in (3, 4, 5, 6):
            gat(kind, r).start()

    def relay2(r):
        await_bytes(xg.at[0:CHUNK, 0:256], f"g1{r}")
        gat(7, r).start()
        gat(8, r).start()

    def rows_of(shard, off, n):
        return pl.ds(pl.multiple_of(shard * 128 + off, 8), n)

    near = (left, right, opp)
    xr_id = at_sp(z * 4 + (xx + 1) % 4)
    xl_id = at_sp(z * 4 + (xx + 3) % 4)
    zr_id = at_sp(((z + 1) % 8) * 4 + xx)
    zl_id = at_sp(((z + 7) % 8) * 4 + xx)
    moves = {"m": (wo.at[:, rows_of(t, 0, 128), :], at_tp(mate))}
    a_own = wo.at[0, rows_of(t, 0, 64), :]
    moves["ar"] = (a_own, at_tp(right))
    moves["al"] = (a_own, at_tp(left))
    moves["afr"] = (wo.at[0, rows_of(left, 0, 32), :], at_tp(right))
    moves["afl"] = (wo.at[0, rows_of(right, 32, 32), :], at_tp(left))
    for j in range(3):
        moves["am", j] = (wo.at[0, rows_of(near[j], 0, 64), :], at_tp(mate))

    def spread_moves(name, w_at, base, piece, place, to_right, to_left):
        def part(shard, off, n):
            return wo.at[w_at, rows_of(shard, base + off, n), :]

        half = piece // 2
        mine = piece * place
        before, after = piece * ((place + 3) % 4), piece * ((place + 1) % 4)
        moves[name, "yr"] = (part(t, mine, piece), at_tp(right))
        moves[name, "yl"] = (part(t, mine, piece), at_tp(left))
        moves[name, "yfr"] = (part(left, mine, half), at_tp(right))
        moves[name, "yfl"] = (part(right, mine + half, half), at_tp(left))
        for j in range(3):
            shard = near[j]
            moves[name, "r", j] = (part(shard, mine, piece), to_right)
            moves[name, "l", j] = (part(shard, mine, piece), to_left)
            moves[name, "fr", j] = (part(shard, before, half), to_right)
            moves[name, "fl", j] = (part(shard, after + half, half), to_left)
            across = piece * ((place + 2) % 4)
            for k, off in enumerate((mine, before, after, across)):
                moves[name, f"m{k}", j] = (part(shard, off, piece), at_tp(mate))

    spread_moves("b", 1, 0, 32, xx, xr_id, xl_id)
    spread_moves("z", 0, 64, 16, zi, zr_id, zl_id)

    def go(name, *tags):
        for tag in tags:
            for key in [k for k in moves if k[:2] == (name, tag)]:
                move(*key).start()

    def landing(key):
        if key == "m":
            return "bm"
        if isinstance(key, str):
            return "a" if key in ("ar", "al") else "af"
        name, tag = key[:2]
        if name == "am":
            return "zm"
        if tag in ("yr", "yl"):
            return name + "y"
        if tag in ("yfr", "yfl"):
            return name + "f"
        if tag in ("r", "l"):
            return name + ("1" if name == "b" and key[2] > 0 else "0")
        return name + ("x" if tag in ("fr", "fl") else "m")

    def move(*key):
        key = key if len(key) > 1 else key[0]
        ref, to = moves[key]
        return send(ref, ref, sem("ms"), sem(landing(key)), to)

    def got(name, rows):
        await_bytes(wo.at[0, 0:rows, :], name)

    xcopy.wait()
    own(0)
    own(1)

    pick = (lax.broadcasted_iota(jnp.int32, (8, 128), 0) == t).astype(BF)
    lane = lax.broadcasted_iota(jnp.int32, (8, 128), 1)
    w[:, 896:1024] = (
        mm(wb[...], jnp.where(lane < 64, pick, 0), TN)
        + mm(wd[...], jnp.where(lane < 64, 0, pick), TN)
    ).astype(BF)
    rate = jnp.exp(jnp.full((1, 128), dlog[t], F32))
    row, col = iotas((BLK, BLK))
    causal = row >= col
    strict = row > col
    tri = causal.astype(F32)
    mn[:, :128] = (row == col).astype(F32)
    mn[:, 128:] = jnp.zeros((BLK, BLK), F32)

    await_bytes(w.at[:, :896], "w")

    def project(r):
        rows = slice(r * CHUNK, (r + 1) * CHUNK)
        xr_ = xg[rows, :]
        xf = xr_.astype(F32)
        inv = lax.rsqrt(jnp.sum(xf * xf, axis=1, keepdims=True) / 2048.0 + NORM)
        raw = []
        for n in range(0, COLS, 256):
            d = jnp.dot(xr_, w[:, n : n + 256], preferred_element_type=F32) * inv
            raw += [d[:, :128], d[:, 128:]]
        q, k, v, dg, gv, gg, cg = [a.astype(BF).astype(F32) for a in raw[:7]]
        qs[rows, :] = unit_rows(q) * (128.0 ** -0.5)
        ks[rows, :] = unit_rows(k)
        vs[rows, :] = v
        dgs[rows, :] = dg * sigmoid(dg)
        cgs[rows, :] = cg * sigmoid(cg)
        turned = pltpu.roll(raw[7], 64, 1)
        low_lanes = lax.broadcasted_iota(jnp.int32, (CHUNK, 128), 1) < 64
        bes[rows, :] = sigmoid(jnp.where(low_lanes, raw[7], turned))
        lds[rows, :] = -rate * softplus(jnp.where(low_lanes, turned, raw[7]))
        below = slice(r * CHUNK + 32, (r + 1) * CHUNK + 32)
        pad[below, :] = (gv * sigmoid(gg)).astype(BF).astype(F32)

    def delta(first, last, mid=None):
        spans = [slice(b * BLK, (b + 1) * BLK) for b in range(first, last)]
        sums, lows, scores = [], [], []
        for rows in spans:
            log = lds[rows, :]
            top = log.astype(BF)
            rest = log - top.astype(F32)
            middle = rest.astype(BF)
            least = (rest - middle.astype(F32)).astype(BF)
            terms = mm(tri, jnp.concatenate([top, middle, least], axis=1))
            total = terms[:, :128] + (terms[:, 128:256] + terms[:, 256:])
            spread = total - total.T
            damp = jnp.where(causal, jnp.exp(jnp.where(causal, spread, 0.0)), 0.0)
            kb = ks[rows, :].astype(BF)
            both = mm(jnp.concatenate([kb, qs[rows, :].astype(BF)], axis=0), kb, NT)
            lows.append(jnp.where(strict, both[:BLK] * bes[rows, :] * damp, 0.0))
            scores.append(both[BLK:] * damp)
            sums.append(total)
        inverses = block_inverse(lows)
        if mid is not None:
            mid()
        later = []
        for rows, total, score, inv in zip(spans, sums, scores, inverses):
            grow = jnp.exp(total)
            kv, be = ks[rows, :], bes[rows, :]
            rhs = jnp.concatenate([vs[rows, :] * be, kv * be * grow], axis=1)
            solved = mm(inv, rhs).astype(BF)
            mixed = mm(score, solved)
            tail = total[BLK - 1 : BLK, :]
            fresh = mm(kv * jnp.exp(tail - total), solved, TN)
            later.append(
                (
                    jnp.concatenate([qs[rows, :] * grow - mixed[:, 128:], fresh[:, 128:]], axis=0),
                    mixed[:, :128], fresh[:, :128], jnp.exp(tail),
                )
            )
        state = mn[...]
        for rows, (lhs, o_here, n_here, fade) in zip(spans, later):
            moved = mm(lhs, state)
            qcs[rows, :] = moved[:BLK, :128]
            ocs[rows, :] = moved[:BLK, 128:] + o_here
            m_next = state[:, :128] * fade - moved[BLK:, :128]
            n_next = state[:, 128:] * fade - moved[BLK:, 128:] + n_here
            state = jnp.concatenate([m_next, n_next], axis=1)
        mn[...] = state

    def arrive(r):
        await_bytes(xg.at[0:CHUNK, 0:1024], f"g2{r}")

    relay1(0)
    own(2)
    relay1(1)
    own(3)
    relay2(0)
    await_bytes(wo.at[:, 0:128, :], "wo")

    arrive(0)
    project(0)
    relay1(2)
    delta(0, 2, lambda: relay2(1))
    relay1(3)
    arrive(1)
    project(1)

    def middle():
        relay2(2)
        go("b", "yr", "yl")
        go("z", "yr", "yl")

    delta(2, 4, middle)
    relay2(3)
    move("m").start()
    arrive(2)
    project(2)
    arrive(3)
    project(3)
    delta(4, 8)
    own_x = mn[...].astype(BF)
    mnx[xx] = own_x

    def xsend(d):
        return send(mnx.at[xx], mnx.at[xx], sem("xs"), sem("xr"),
                    at_sp(z * 4 + (xx + d) % 4))

    for d in (1, 2, 3):
        xsend(d).start()
    halo_s[...] = pad[ROWS : ROWS + 32, :].astype(BF)
    hcopy = send(halo_s, halo_r, sem("hs"), sem("hr"), at_sp((sp + 1) % 32))

    @pl.when(z < 7)
    def _():
        pl.semaphore_wait(
            ack, 3 - zi + 1 + count(z == 0, xx == 3) + 4 * count(z == 3)
        )

    @pl.when(sp < 31)
    def _():
        hcopy.start()

    for name, rows in (("b", 64), ("z", 32)):
        got(name + "y", rows)
        go(name, "yfr", "yfl")
        for j in (0, 1):
            move(name, "r", j).start()
            move(name, "l", j).start()
            move(name, "m0", j).start()

    tapf = taps[...].astype(F32)

    def conv_rows(i):
        acc = jnp.zeros((64, 128), F32)
        for j in range(TAPS):
            acc = acc + pad[pl.ds(i * 64 + 2 + j, 64), :] * tapf[j : j + 1, :]
        filt[pl.ds(pl.multiple_of(i * 64, 64), 64), :] = acc

    @pl.loop(1, ROWS // 64)
    def _(i):
        conv_rows(i)

    @pl.when(sp > 0)
    def _():
        hcopy.wait_recv()

    keep = (sp > 0).astype(F32)
    pad[0:32, :] = halo_r[...].astype(F32) * keep
    conv_rows(0)
    for b in range(ROWS // BLK):
        lanes = slice(b * BLK, (b + 1) * BLK)
        ft = filt[lanes, :].T
        sts[0:1, lanes] = jnp.sum(ft, axis=0, keepdims=True)
        sts[1:2, lanes] = jnp.sum(ft * ft, axis=0, keepdims=True)

    def ssend(d):
        return send(sts, str_.at[t], sem("ss"), sem("sr"), at_tp((t + d) % 8))

    for d in range(1, 8):
        ssend(d).start()
    str_[t] = sts[...]

    def chain(slots, mine):
        total = slots[0].astype(F32)
        m_in = jnp.where(mine > 0, total[:, :128], (row == col).astype(F32))
        n_in = jnp.where(mine > 0, total[:, 128:], 0.0)
        for k in (1, 2, 3):
            piece = slots[k]
            moved = mm(piece[:, :128], total)
            total = jnp.concatenate(
                [moved[:, :128], moved[:, 128:] + piece[:, 128:].astype(F32)], axis=1
            )
            if k < 3:
                m_in = jnp.where(mine > k, total[:, :128], m_in)
                n_in = jnp.where(mine > k, total[:, 128:], n_in)
        return m_in, n_in, total

    got("zf", 16)
    for tag in ("r", "l", "m0"):
        move("z", tag, 2).start()
    await_bytes(mnx.at[0:3], "xr")
    mxp, nxp, xtotal = chain(mnx, xx)
    mnz[zi] = xtotal.astype(BF)

    def zsend(d):
        return send(mnz.at[zi], mnz.at[zi], sem(f"zs{d}"), sem(f"zr{d}"), at_sp((sp + 4 * d) % 32))

    def upward(d, act):
        @pl.when(zi + d < 4)
        def _():
            act(zsend(d))

    for d in (1, 2, 3):
        upward(d, lambda copy: copy.start())

    got("bf", 32)
    for tag in ("r", "l", "m0"):
        move("b", tag, 2).start()
    move("ar").start()
    move("al").start()
    got("b0", 64)
    for tag in ("fr", "fl", "m1", "m2"):
        move("b", tag, 0).start()
    await_bytes(str_.at[0:7], "sr")
    both = str_[0]
    for k in range(1, 8):
        both = both + str_[k]
    center = both[0:1, :] / 1024.0
    variance = jnp.maximum(both[1:2, :] / 1024.0 - center * center, 0.0)
    scale = lax.rsqrt(variance + VAR)
    for b in range(ROWS // BLK):
        lanes = slice(b * BLK, (b + 1) * BLK)
        cen = jnp.broadcast_to(center[:, lanes], (BLK, BLK)).T
        sca = jnp.broadcast_to(scale[:, lanes], (BLK, BLK)).T
        normed = (filt[lanes, :] - cen) * sca * lng[...] + lns[...]
        cms[lanes, :] = (normed * sigmoid(normed) * cgs[lanes, :]).astype(BF)

    def a2a(src, dst, s_sem, r_sem, d):
        to = (t + d) % 8
        rows = pl.ds(pl.multiple_of(to * BLK, BLK), BLK)
        return send(src.at[rows, :], dst.at[t], sem(s_sem), sem(r_sem), at_tp(to))

    for d in FAR_FIRST:
        a2a(cms, cmr, "cs", "cr", d).start()
    cmr[t] = cms[own_rows, :]

    for d in (1, 2, 3):
        @pl.when(zi - d >= 0)
        def _():
            zsend(d).wait_recv()

    mzp, nzp, ztotal = chain(mnz, zi)
    s4s[...] = ztotal[:, 128:].astype(BF)

    def fcopy(d):
        return send(s4s, s4r, sem("fs"), sem("fr"), at_sp((sp + 4 * d) % 32))

    @pl.when(z == 3)
    def _():
        for d in (4, 3, 2, 1):
            fcopy(d).start()

    moved = mm(mxp, jnp.concatenate([mzp, nzp], axis=1))
    mpre, npre = moved[:, :128], moved[:, 128:] + nxp
    got("b1", 128)
    for j in (1, 2):
        for tag in ("fr", "fl", "m1", "m2"):
            move("b", tag, j).start()
    got("z0", 96)
    go("z", "fr", "fl", "m1", "m2")
    got("a", 128)
    for key in ("afr", "afl"):
        move(key).start()
    move("am", 0).start()
    move("am", 1).start()
    @pl.when(z >= 4)
    def _():
        fcopy(1).wait_recv()

    begin = s4r[...].astype(F32) * (zq > 0).astype(F32)
    carried = mm(mpre, begin) + npre

    for i, d in enumerate(FAR_FIRST + (0,)):
        lanes = pl.ds(pl.multiple_of(lax.rem(t + d, 8) * BLK, BLK), BLK)
        o = ocs[lanes, :] + mm(qcs[lanes, :], carried)
        o = o * lax.rsqrt(jnp.mean(o * o, axis=-1, keepdims=True) + NORM) * hgain[...]
        dms[lanes, :] = (o * dgs[lanes, :]).astype(BF)
        if i in (3, 7):
            for e in FAR_FIRST[max(i - 4, 0) : i]:
                a2a(dms, dmr, "ds", "dr", e).start()
    dmr[t] = dms[own_rows, :]

    got("bx", 96)
    go("b", "m3")
    await_bytes(cmr.at[0:7], "cr")
    got("bm", 640)
    lhs_c = jnp.concatenate([cmr[k] for k in range(8)], axis=1)

    def conv_part(n):
        lanes = pl.ds(pl.multiple_of(n * 256, 256), 256)
        half[n] = jnp.dot(lhs_c, wo[1, :, lanes], preferred_element_type=F32)

    @pl.loop(0, 4)
    def _(n):
        conv_part(n)

    got("af", 64)
    move("am", 2).start()
    got("zx", 48)
    go("z", "m3")
    @pl.loop(4, 8)
    def _(n):
        conv_part(n)

    got("zm", 384)
    await_bytes(dmr.at[0:7], "dr")

    lhs_d = jnp.concatenate([dmr[k] for k in range(8)], axis=1)

    def ocopy(n):
        lanes = pl.ds(pl.multiple_of(n * 256, 256), 256)
        return pltpu.make_async_copy(stage.at[n], out.at[:, lanes], sem("out"))

    @pl.loop(0, 8)
    def _(n):
        lanes = pl.ds(pl.multiple_of(n * 256, 256), 256)
        acc = jnp.dot(lhs_d, wo[0, :, lanes], preferred_element_type=F32)
        stage[n] = (acc + half[n]).astype(BF)
        ocopy(n).start()

    await_bytes(stage, "out")
    await_bytes(xg.at[0:896, :], "gs")
    await_bytes(wo.at[:, 0:896, :], "ms")
    await_bytes(mnx.at[0:3], "xs")
    for d in (1, 2, 3):
        upward(d, lambda copy: copy.wait_send())

    @pl.when(z == 3)
    def _():
        await_bytes(mnx.at[0:2], "fs")


    @pl.when(sp < 31)
    def _():
        await_bytes(halo_s, "hs")

    await_bytes(str_.at[0:7], "ss")
    await_bytes(dmr.at[0:7], "ds")
    await_bytes(cmr.at[0:7], "cs")


def local(*args):
    (tokens, w_query, w_key, w_value, w_delta_gate, w_glu_value, w_glu_gate, w_conv_gate,
     w_beta, w_decay, decay_log, head_gain, conv_taps, ln_gain, ln_shift, out_delta,
     out_conv) = args
    vm = pl.BlockSpec(memory_space=pltpu.VMEM)
    hb = pl.BlockSpec(memory_space=pl.ANY)
    sm = pl.BlockSpec(memory_space=pltpu.SMEM)
    big = lambda kind: pltpu.VMEM((ROWS, 128), kind)
    dma = pltpu.SemaphoreType.DMA
    return pl.pallas_call(
        kernel,
        out_shape=jax.ShapeDtypeStruct((BLK, 2048), BF),
        in_specs=[hb] * 8 + [vm, vm, sm] + [vm] * 4 + [hb, hb],
        out_specs=hb,
        scratch_shapes=[
            pltpu.VMEM((ROWS, 2048), BF),
            pltpu.VMEM((2048, COLS), BF),
            pltpu.VMEM((2, 1024, 2048), BF),
            big(F32), big(F32), big(F32), big(F32), big(F32), big(F32), big(F32),
            pltpu.VMEM((ROWS + 32, 128), F32),
            big(F32), big(F32), big(F32),
            pltpu.VMEM((BLK, 256), F32),
            pltpu.VMEM((4, BLK, 256), BF),
            pltpu.VMEM((4, BLK, 256), BF),
            pltpu.VMEM((BLK, BLK), BF),
            pltpu.VMEM((BLK, BLK), BF),
            pltpu.VMEM((32, 128), BF),
            pltpu.VMEM((32, 128), BF),
            pltpu.VMEM((2, ROWS), F32),
            pltpu.VMEM((8, 2, ROWS), F32),
            big(BF), big(BF),
            pltpu.VMEM((8, BLK, BLK), BF),
            pltpu.VMEM((8, BLK, BLK), BF),
            pltpu.VMEM((8, BLK, 256), BF),
            pltpu.VMEM((8, BLK, 256), F32),
            dma((len(SEMS),)),
            pltpu.SemaphoreType.REGULAR,
        ],
        compiler_params=pltpu.CompilerParams(
            collective_id=0, has_side_effects=True, vmem_limit_bytes=60 * 1024 * 1024
        ),
        name="layer",
    )(
        tokens, w_query, w_key, w_value, w_delta_gate, w_glu_value, w_glu_gate, w_conv_gate,
        w_beta.T, w_decay.T, decay_log, head_gain.reshape(1, 128), conv_taps,
        ln_gain.reshape(1, 128), ln_shift.reshape(1, 128), out_delta, out_conv,
    )


def solution(mesh):
    cut = P(None, "tp")
    placed = (P("sp", "tp"),) + (cut,) * 7 + (P(),) * 4 + (
        cut, P("tp"), P("tp"), P("tp", None), P("tp", None),
    )
    return jax.shard_map(
        local, mesh=mesh, in_specs=placed, out_specs=P(("sp", "tp"), None), check_vma=False
    )
```
